32 devices in a mesh: ep: 8 (over z, core), tp: 4 (over y, x).
Axes of the slice: x: 2, y: 2, z: 4, core: 2. Of those that a mesh axis runs over, the one named last changes fastest.
Arguments:
- query_pairs: bfloat16 [3072, 2048], P('ep', 'tp'), may hold values from -64 to 64
- key_pairs: bfloat16 [3072, 2048], P('ep', 'tp'), may hold values from -64 to 64
- value_rows: bfloat16 [3072, 2048], P('ep', 'tp'), may hold values from -6 to 6
- head_lambda: float32 [16], P('tp'), may hold values from 0.3 to 0.8
- head_gain: float32 [128], replicated, may hold values from 0.1 to 1.9
- out_weight: bfloat16 [2048, 2048], P('tp'), may hold values from -0.1875 to 0.1875
- moe_input: bfloat16 [1280, 2048], P('ep'), may hold values from -6 to 6
- ffn_gain: float32 [2048], replicated, may hold values from 0.1 to 1.9
- routes: int32 [1280, 2], P('ep'), may hold values from 0 to 7, all different within a row; in each aligned block of 160 rows (0 to 159, 160 to 319, ...) at most 50 rows name the same one
- route_weight: float32 [1280, 2], P('ep'), may hold values from 0.25 to 2.5
- gate_weight: bfloat16 [8, 2048, 2048], P('ep', None, 'tp'), may hold values from -0.125 to 0.125
- up_weight: bfloat16 [8, 2048, 2048], P('ep', None, 'tp'), may hold values from -0.125 to 0.125
- down_weight: bfloat16 [8, 2048, 2048], P('ep', 'tp'), may hold values from -0.1875 to 0.1875
- shared_gate: bfloat16 [2048, 2048], P(None, 'tp'), may hold values from -0.125 to 0.125
- shared_up: bfloat16 [2048, 2048], P(None, 'tp'), may hold values from -0.125 to 0.125
- shared_down: bfloat16 [2048, 2048], P('tp'), may hold values from -0.1875 to 0.1875
Outputs:
- attn_out: bfloat16 [3072, 2048], P('ep', 'tp')
- moe_out: bfloat16 [1280, 2048], P('ep', 'tp')
The draws below stay inside these ranges and needn't reach their ends.
Inputs may be any that keep to these rules, and one draw needn't show every extreme that they name: `routes`: in each aligned block of 160 rows (the rows of one device along ep) no expert is named more than 50 times, a bound that some block reaches; a row names 2 different experts.
All inputs are finite; a program needn't handle non-finite values.
Results may differ from the reference program's by a relative error of at most 0.017.
The reference program's roundings to bfloat16 on the way count: a program that leaves them out, or rounds other values in their place, can miss the bound.
Values may be sent and summed in bfloat16 or wider, within the bound.
No kernel may reach another device: no remote copies, remote signals or barrier semaphores. Data moves between devices by JAX's collectives and lax.ppermute only.
A program may use at most 64 MiB of HBM per device.

```python
import math
import jax
import jax.numpy as jnp
import numpy as np
from jax import lax

D = 2048
HEADS = 16
HEAD = 64
VHEAD = 128
FF = 2048
SFF = 2048
TOP_K = 2
KEY_BLOCK = 128
TOK_B = 160
TOKENS_A = 3072
TOKENS_B = 1280
EXPERTS = 8
CAP = 50
N_TP = 4


def paired_draw(key):
    draw_shape = (TOKENS_A, HEADS, 2, HEAD)
    queries = 1.3 * jax.random.truncated_normal(jax.random.fold_in(key, 101), -4.0, 4.0, draw_shape, jnp.float32)
    keyset = 1.3 * jax.random.truncated_normal(jax.random.fold_in(key, 102), -4.0, 4.0, draw_shape, jnp.float32)
    return (jnp.clip(queries, -64.0, 64.0), jnp.clip(keyset, -64.0, 64.0))


def draw_query_pairs(key, part):
    return paired_draw(key)[0].reshape(TOKENS_A, HEADS * 2 * HEAD).astype(jnp.bfloat16)


def draw_key_pairs(key, part):
    return paired_draw(key)[1].reshape(TOKENS_A, HEADS * 2 * HEAD).astype(jnp.bfloat16)


def with_spikes(entries, rng, source, target, blocks, factor):
    owner, partner = [(jnp.arange(entries.shape[axis_at]) // (entries.shape[axis_at] // blocks)).reshape([-1 if axis == axis_at else 1 for axis in range(entries.ndim)]) for axis_at in (source, target)]
    chosen = jax.random.permutation(rng, blocks)[partner]
    strong = (owner == chosen) | (owner == (partner + blocks // 2) % blocks)
    return jnp.where(strong, factor * entries, entries)


def level_of(key, dims, split, smallest, high):
    level, own = 1.0, jax.random.fold_in(key, 6)
    for dim, parts in split:
        draws = jnp.exp(jax.random.uniform(jax.random.fold_in(own, dim), (parts,), jnp.float32, smallest / len(split), high / len(split)))
        level = level * jnp.repeat(draws, dims[dim] // parts).reshape([-1 if axis == dim else 1 for axis in range(len(dims))])
    return level


def routed_block(own_key, own, number, rows, count, top, limit, lean):
    order = jax.random.permutation(own_key, count)
    heavy_load, usual = portions_of(count, rows * top, limit, lean, True), portions_of(count, rows * top, limit, lean, False)
    places = jnp.arange(count)

    def named(tallies, turn):
        used = int((tallies > 0).sum())
        fixed = max(1, used // 4)
        passed = fixed + (places - fixed + turn * (used - fixed)) % max(1, count - fixed)
        return jnp.zeros((count,), jnp.int32).at[order[jnp.where(places < fixed, places, passed)]].set(jnp.asarray(tallies, jnp.int32))

    tallies = jnp.where(number % 4 == 0, named(heavy_load, number // 4), named(usual, number - number // 4 - 1))
    mixed = jax.random.permutation(jax.random.fold_in(own, 3), count)
    source_of, taker = mixed[0:count // 2 * 2:2], mixed[1:count // 2 * 2:2]
    slack = jnp.minimum(tallies[source_of] - 1, limit - tallies[taker]) // 2
    slack = jnp.where((source_of == order[0]) | (taker == order[0]) | (tallies[taker] == 0), 0, jnp.maximum(slack, 0))
    passed = jax.random.randint(jax.random.fold_in(own, 4), (count // 2,), 0, 1 << 20) % (slack + 1)
    tallies = tallies.at[source_of].add(-passed).at[taker].add(passed)
    labels = jnp.searchsorted(jnp.cumsum(tallies), jnp.arange(rows * top), side="right").astype(jnp.int32)
    grid = labels.reshape(top, rows).T
    grid = grid[jax.random.permutation(jax.random.fold_in(own, 1), rows)]
    turn = jax.random.randint(jax.random.fold_in(own, 2), (rows, 1), 0, top)
    return jnp.take_along_axis(grid, (jnp.arange(top)[None, :] + turn) % top, axis=1)


def portions_of(number_of, total, limit, slope, full):
    weights = [(1 << 20) // math.isqrt(standing ** slope) + 1 for standing in range(1, number_of + 1)]
    largest = limit if full else min(limit, max(-(-total // number_of), total * weights[0] // sum(weights)))
    least = 1 if total - largest >= number_of - 1 else 0
    counts, spare = [largest] + [least] * (number_of - 1), total - largest - least * (number_of - 1)
    while spare > 0:
        free = [i for i in range(1, number_of) if counts[i] < largest] or [i for i in range(1, number_of) if counts[i] < limit]
        mass, remaining = sum([weights[i] for i in free]), spare
        for i in free:
            more = min(limit - counts[i], max(1, remaining * weights[i] // mass), spare)
            counts[i] = counts[i] + more
            spare = spare - more
    return np.array(counts)


def scatter_about(rng, dims, scale, bound, shards=(), held_as=jnp.bfloat16):
    loudness = level_of(rng, dims, shards, -0.22, 0.18) if shards else 1.0
    drawn = jax.random.normal(rng, dims, jnp.float32) * scale * loudness
    return jnp.minimum(jnp.maximum(drawn, -bound), bound).astype(held_as)


def bell_draw_with(stream_key, shape, width, limit, shards, heavy, kind=jnp.bfloat16):
    values = width * jax.random.normal(stream_key, shape, jnp.float32)
    if shards:
        values = values * level_of(stream_key, shape, shards, -0.22, 0.18)
    return jnp.clip(with_spikes(values, jax.random.fold_in(stream_key, 3), *heavy), -limit, limit).astype(kind)


def setup_inputs(seed: int = 0) -> dict:
    streams_of = jax.random.split(jax.random.key(seed), 17)
    query_pairs = draw_query_pairs(jax.random.fold_in(streams_of[16], 71), 0)
    key_pairs = draw_key_pairs(jax.random.fold_in(streams_of[16], 71), 0)
    value_rows = scatter_about(streams_of[2], (TOKENS_A, HEADS * VHEAD), 1.0, 6.0, ((0, 8), (1, 4)))
    head_lambda = jnp.clip(0.3 + 0.5 * jax.random.uniform(streams_of[3], (HEADS,), jnp.float32) ** level_of(streams_of[3], (HEADS,), ((0, 4),), -0.2, 0.2), 0.3, 0.8)
    head_gain = jnp.clip(1.0 + 0.18 * jax.random.normal(streams_of[4], (VHEAD,), jnp.float32), 0.1, 1.9)
    out_weight = bell_draw_with(streams_of[5], (HEADS * VHEAD, D), (HEADS * VHEAD) ** -0.5, 0.1875, ((0, 4),), (0, 1, 4, 2.0))
    moe_input = scatter_about(streams_of[6], (TOKENS_B, D), 1.0, 6.0, ((0, 8),))
    ffn_gain = jnp.clip(1.0 + 0.18 * jax.random.normal(streams_of[7], (D,), jnp.float32), 0.1, 1.9)
    routes_keys = jax.random.split(jax.random.fold_in(streams_of[8], 1), TOKENS_B // TOK_B)
    routes_turns = jax.random.permutation(jax.random.fold_in(streams_of[8], 3), TOKENS_B // TOK_B)
    routes = jax.vmap(lambda own, number: routed_block(jax.random.fold_in(streams_of[8], 2), own, number, TOK_B, EXPERTS, TOP_K, CAP, 1))(routes_keys, routes_turns).reshape((TOKENS_B, TOP_K))
    route_weight = jnp.clip(jnp.exp(math.log(2.5) - 2.3025851 * jax.random.uniform(streams_of[9], (TOKENS_B, TOP_K), jnp.float32) ** level_of(streams_of[9], (TOKENS_B, TOP_K), ((0, 8),), -0.2, 0.2)), 0.25, 2.5)
    gate_weight = scatter_about(streams_of[10], (EXPERTS, D, FF), D ** -0.5, 0.125, ((0, 8), (2, 4)))
    up_weight = scatter_about(streams_of[11], (EXPERTS, D, FF), D ** -0.5, 0.125, ((0, 8), (2, 4)))
    down_weight = bell_draw_with(streams_of[12], (EXPERTS, FF, D), FF ** -0.5, 0.1875, ((0, 8), (1, 4)), (1, 2, 4, 2.0))
    shared_gate = scatter_about(streams_of[13], (D, SFF), D ** -0.5, 0.125, ((1, 4),))
    shared_up = scatter_about(streams_of[14], (D, SFF), D ** -0.5, 0.125, ((1, 4),))
    shared_down = bell_draw_with(streams_of[15], (SFF, D), SFF ** -0.5, 0.1875, ((0, 4),), (0, 1, 4, 2.0))
    return {"query_pairs": query_pairs, "key_pairs": key_pairs, "value_rows": value_rows, "head_lambda": head_lambda, "head_gain": head_gain, "out_weight": out_weight, "moe_input": moe_input, "ffn_gain": ffn_gain, "routes": routes, "route_weight": route_weight, "gate_weight": gate_weight, "up_weight": up_weight, "down_weight": down_weight, "shared_gate": shared_gate, "shared_up": shared_up, "shared_down": shared_down}


theta_base = 500000.0
norm_eps = 1e-06
masked_low = -1e+30

def rotate(inputs, positions):
    half_size = inputs.shape[-1] // 2
    frequency = theta_base ** (-(jnp.arange(half_size, dtype=jnp.float32) * 2.0) / inputs.shape[-1])
    angles = positions.astype(jnp.float32)[:, None] * frequency[None, :]
    cosine = jnp.cos(angles)[:, None, None, :]
    sine_part = jnp.sin(angles)[:, None, None, :]
    front_half = inputs[..., :half_size]
    back_half = inputs[..., half_size:]
    return jnp.concatenate([front_half * cosine - back_half * sine_part, back_half * cosine + front_half * sine_part], axis=-1)

def attention(query_pairs, key_pairs, value_rows, head_lambda, head_gain, out_weight):
    total_rows = query_pairs.shape[0]
    head_count = head_lambda.shape[0]
    head_size = query_pairs.shape[1] // (2 * head_count)
    value_size = value_rows.shape[1] // head_count
    positions = jnp.arange(total_rows, dtype=jnp.int32)
    rot_queries = rotate(query_pairs.astype(jnp.float32).reshape(total_rows, head_count, 2, head_size), positions).astype(jnp.bfloat16)
    rot_keys = rotate(key_pairs.astype(jnp.float32).reshape(total_rows, head_count, 2, head_size), positions).astype(jnp.bfloat16)
    key_blocks = total_rows // KEY_BLOCK
    block_keys = rot_keys.reshape(key_blocks, KEY_BLOCK, head_count, 2, head_size).astype(jnp.float32)
    block_values = value_rows.reshape(key_blocks, KEY_BLOCK, head_count, value_size).astype(jnp.float32)
    key_positions = positions.reshape(key_blocks, KEY_BLOCK)
    query_block = math.gcd(total_rows, 256)
    query_count = total_rows // query_block

    def one_block(inputs):
        block_queries, query_positions = inputs
        scores = jnp.einsum('qhmd,bkhmd->hmqbk', block_queries.astype(jnp.float32), block_keys) * head_size ** (-0.5)
        allowed = key_positions[None, :, :] <= query_positions[:, None, None]
        scores = jnp.where(allowed, scores, masked_low)
        block_max = lax.optimization_barrier(jnp.max(scores, axis=-1))
        weights = jnp.where(allowed, jnp.exp(scores - block_max[..., None]), 0.0)
        block_sum = lax.optimization_barrier(jnp.sum(weights, axis=-1))
        rounded = lax.optimization_barrier(weights.astype(jnp.bfloat16)).astype(jnp.float32)
        block_out = jnp.einsum('hmqbk,bkhc->hmqbc', rounded, block_values)
        row_max = lax.optimization_barrier(jnp.max(block_max, axis=-1, keepdims=True))
        rescale = jnp.exp(block_max - row_max)
        summed = lax.optimization_barrier(jnp.sum(rescale * block_sum, axis=-1))
        combined = lax.optimization_barrier(jnp.sum(rescale[..., None] * block_out, axis=-2))
        return combined / summed[..., None]
    outputs = lax.map(one_block, (rot_queries.reshape(query_count, query_block, head_count, 2, head_size), positions.reshape(query_count, query_block)))
    difference = outputs[:, :, 0] - head_lambda[None, :, None, None] * outputs[:, :, 1]
    inverse_rms = lax.rsqrt(lax.optimization_barrier(jnp.mean(difference * difference, axis=-1, keepdims=True)) + norm_eps)
    normed = (difference * inverse_rms * head_gain.astype(jnp.float32)).astype(jnp.bfloat16)
    normed = normed.transpose(0, 2, 1, 3).reshape(total_rows, head_count * value_size)
    group_cols = head_count * value_size // N_TP
    grouped = normed.reshape(total_rows, N_TP, group_cols).transpose(1, 0, 2)
    weight_groups = out_weight.reshape(N_TP, group_cols, out_weight.shape[1])

    def add_group(running, block_parts):
        partial_out = jnp.dot(block_parts[0], block_parts[1], preferred_element_type=jnp.float32)
        return (running + lax.optimization_barrier(partial_out.astype(jnp.bfloat16)).astype(jnp.float32), None)
    result, _ = lax.scan(add_group, jnp.zeros((total_rows, out_weight.shape[1]), jnp.float32), (grouped, weight_groups))
    return result.astype(jnp.bfloat16)

def swiglu_blocks(inputs, gate_w, up_w, down_w):
    model_width = gate_w.shape[0]
    block_width = gate_w.shape[1] // N_TP
    gate_blocks = gate_w.reshape(model_width, N_TP, block_width).transpose(1, 0, 2)
    up_blocks = up_w.reshape(model_width, N_TP, block_width).transpose(1, 0, 2)
    down_blocks = down_w.reshape(N_TP, block_width, down_w.shape[1])

    def add_block(running, block_parts):
        gate_part = jnp.dot(inputs, block_parts[0], preferred_element_type=jnp.float32)
        up_part = jnp.dot(inputs, block_parts[1], preferred_element_type=jnp.float32)
        hidden = (jax.nn.silu(gate_part) * up_part).astype(jnp.bfloat16)
        partial_out = jnp.dot(hidden, block_parts[2], preferred_element_type=jnp.float32)
        return (running + lax.optimization_barrier(partial_out.astype(jnp.bfloat16)).astype(jnp.float32), None)
    result, _ = lax.scan(add_block, jnp.zeros((inputs.shape[0], down_w.shape[1]), jnp.float32), (gate_blocks, up_blocks, down_blocks))
    return result

def mixture(moe_input, ffn_gain, routes, route_weight, gate_weight, up_weight, down_weight, shared_gate, shared_up, shared_down):
    row_values = moe_input.astype(jnp.float32)
    inverse_rms = lax.rsqrt(lax.optimization_barrier(jnp.mean(row_values * row_values, axis=-1, keepdims=True)) + norm_eps)
    normed = (row_values * inverse_rms * ffn_gain.astype(jnp.float32)).astype(jnp.bfloat16)
    total_rows = normed.shape[0]
    experts = gate_weight.shape[0]
    blocks = total_rows // TOK_B
    flat_routes = routes.reshape(blocks, TOK_B * TOP_K)
    onehot = (flat_routes[..., None] == jnp.arange(experts, dtype=jnp.int32)).astype(jnp.int32)
    slot_rank = lax.optimization_barrier(jnp.sum((jnp.cumsum(onehot, axis=1) - 1) * onehot, axis=-1)).astype(jnp.int32)
    token_ids = jnp.arange(blocks, dtype=jnp.int32)[:, None] * TOK_B + jnp.arange(TOK_B * TOP_K, dtype=jnp.int32)[None, :] // TOP_K
    source_ids = jnp.broadcast_to(jnp.arange(blocks, dtype=jnp.int32)[:, None], flat_routes.shape)
    slot_table = jnp.full((experts, blocks, CAP), total_rows, jnp.int32).at[flat_routes, source_ids, slot_rank].set(token_ids)
    padded = jnp.concatenate([normed, jnp.zeros((1, normed.shape[1]), jnp.bfloat16)], axis=0)

    def one_expert(inputs):
        chosen = padded[inputs[0].reshape(-1)]
        return swiglu_blocks(chosen, inputs[1], inputs[2], inputs[3]).astype(jnp.bfloat16)
    expert_out = lax.map(one_expert, (slot_table, gate_weight, up_weight, down_weight))
    expert_out = expert_out.reshape(experts, blocks, CAP, normed.shape[1])
    block_index = (jnp.arange(total_rows, dtype=jnp.int32) // TOK_B)[:, None]
    picked = expert_out[routes, block_index, slot_rank.reshape(total_rows, TOP_K)]
    shared_sum = swiglu_blocks(normed, shared_gate, shared_up, shared_down)
    combined = lax.optimization_barrier(jnp.sum(route_weight[..., None] * picked.astype(jnp.float32), axis=1)) + shared_sum
    return combined.astype(jnp.bfloat16)

def reference(query_pairs, key_pairs, value_rows, head_lambda, head_gain, out_weight, moe_input, ffn_gain, routes, route_weight, gate_weight, up_weight, down_weight, shared_gate, shared_up, shared_down):
    attn_out = attention(query_pairs, key_pairs, value_rows, head_lambda, head_gain, out_weight)
    moe_out = mixture(moe_input, ffn_gain, routes, route_weight, gate_weight, up_weight, down_weight, shared_gate, shared_up, shared_down)
    return (attn_out, moe_out)
```

```python
import jax
import jax.numpy as jnp
from jax import lax
from jax.experimental import pallas as pl
from jax.experimental.pallas import tpu as pltpu
from jax.sharding import PartitionSpec as P

TOP_K = 2
KEY_BLOCK = 128

theta_base = 500000.0
norm_eps = 1e-06
masked_low = -1e30
LOG2E = 1.4426950408889634

VM = pl.BlockSpec(memory_space=pltpu.VMEM)
SM = pl.BlockSpec(memory_space=pltpu.SMEM)
ANY = pl.BlockSpec(memory_space=pl.ANY)


def sds(shape, dtype=jnp.bfloat16):
    return jax.ShapeDtypeStruct(shape, dtype)


def cost(flops):
    return pl.CostEstimate(flops=int(flops), bytes_accessed=0, transcendentals=0)


def dispatch_kernel(where, rows, gain, routes, routes_t, xn_out, slots_out, *parts, cap, experts):
    z, core, ti = where[0], where[1], where[2]
    tokens = rows.shape[0]
    values = rows[...].astype(jnp.float32)
    inverse = lax.rsqrt(jnp.mean(values * values, axis=-1, keepdims=True) + norm_eps)
    xn_out[...] = (values * inverse * gain[...]).astype(jnp.bfloat16)
    group = 2 * cap
    t_row = lax.broadcasted_iota(jnp.int32, (tokens, tokens), 0)
    t_col = lax.broadcasted_iota(jnp.int32, (tokens, tokens), 1)
    e_row = lax.broadcasted_iota(jnp.int32, (experts, tokens), 0)
    before = (t_row < t_col).astype(jnp.float32).astype(jnp.bfloat16)
    hit_t = [(e_row == routes_t[k : k + 1, :]).astype(jnp.float32) for k in range(TOP_K)]
    count_t = jnp.dot(
        (hit_t[0] + hit_t[1]).astype(jnp.bfloat16), before, preferred_element_type=jnp.float32
    )
    e_col = lax.broadcasted_iota(jnp.int32, (tokens, experts), 1)
    after = (t_row > t_col).astype(jnp.float32).astype(jnp.bfloat16)
    hit = [(e_col == routes[:, k : k + 1]).astype(jnp.float32) for k in range(TOP_K)]
    count = jnp.dot(after, (hit[0] + hit[1]).astype(jnp.bfloat16), preferred_element_type=jnp.float32)
    slot_t = []
    for k in range(TOP_K):
        expert = routes_t[k : k + 1, :]
        rank = jnp.sum(count_t * hit_t[k], axis=0, keepdims=True).astype(jnp.int32)
        slot_t.append(((expert // 2) ^ z) * group + ((expert % 2) ^ core) * cap + rank)
        expert = routes[:, k : k + 1]
        rank = jnp.sum(count * hit[k], axis=1, keepdims=True).astype(jnp.int32)
        slots_out[:, k : k + 1] = ((expert // 2) ^ z) * group + ((expert % 2) ^ core) * cap + rank
    width = parts[0].shape[1]
    mine = xn_out[:, pl.ds(pl.multiple_of(ti * width, width), width)]
    for s, part in enumerate(parts):
        slot_row = lax.broadcasted_iota(jnp.int32, (group, tokens), 0) + s * group
        pick = (slot_row == slot_t[0]) | (slot_row == slot_t[1])
        pick = pick.astype(jnp.float32).astype(jnp.bfloat16)
        part[...] = jnp.dot(pick, mine, preferred_element_type=jnp.float32).astype(jnp.bfloat16)


def expert_kernel(where, *refs, pieces, outs):
    ti = where[0]
    xs, (gate_w, up_w, down_w), ys = refs[:pieces], refs[pieces : pieces + 3], refs[pieces + 3 :]
    width = xs[0].shape[1]
    gate = up = None
    for s in range(pieces):
        if pieces == 1:
            wg, wu = gate_w[...], up_w[...]
        else:
            at = pl.ds(pl.multiple_of((ti ^ s) * width, width), width)
            wg, wu = gate_w[at, :], up_w[at, :]
        x = xs[s][...]
        g = jnp.dot(x, wg, preferred_element_type=jnp.float32)
        u = jnp.dot(x, wu, preferred_element_type=jnp.float32)
        gate = g if gate is None else gate + g
        up = u if up is None else up + u
    hidden = (gate / (1.0 + jnp.exp(-gate)) * up).astype(jnp.bfloat16)
    cols = ys[0].shape[1]
    for s in range(outs):
        at = pl.ds(pl.multiple_of((ti ^ s) * cols, cols), cols)
        ys[s][...] = jnp.dot(hidden, down_w[:, at], preferred_element_type=jnp.float32).astype(
            jnp.bfloat16
        )


def run_expert(ti, xs, gate_w, up_w, down_w, tp, name):
    rows = xs[0].shape[0]
    width, hidden = gate_w.shape
    cols = down_w.shape[1] // tp
    return pl.pallas_call(
        lambda *refs: expert_kernel(*refs, pieces=len(xs), outs=tp),
        out_shape=[sds((rows, cols))] * tp,
        in_specs=[SM] + [VM] * (len(xs) + 3),
        out_specs=[VM] * tp,
        cost_estimate=cost(6 * rows * width * hidden),
        name=name,
    )(ti.reshape(1), *xs, gate_w, up_w, down_w)


def combine_kernel(slots, weights, *refs, count):
    back, shared, out = refs[:count], refs[count:-1], refs[-1]
    tokens = slots.shape[0]
    group = back[0].shape[0]
    total = None
    for part in shared:
        part = part[...].astype(jnp.float32)
        total = part if total is None else total + part
    picked = [None] * TOP_K
    for s in range(count):
        slot_col = lax.broadcasted_iota(jnp.int32, (tokens, group), 1) + s * group
        rows = back[s][...]
        for k in range(TOP_K):
            pick = (slot_col == slots[:, k : k + 1]).astype(jnp.float32).astype(jnp.bfloat16)
            term = jnp.dot(pick, rows, preferred_element_type=jnp.float32)
            picked[k] = term if picked[k] is None else picked[k] + term
    routed = weights[:, 0:1] * picked[0]
    for k in range(1, TOP_K):
        routed = routed + weights[:, k : k + 1] * picked[k]
    out[...] = (routed + total).astype(jnp.bfloat16)


def rope_kernel(where, q, k, v, cosine, sine, *outs, size):
    z = where[0]
    rows = q.shape[0]
    both = cosine.shape[1]
    half = size // 2
    lane = lax.broadcasted_iota(jnp.int32, (rows, both), 1)
    front = (lane % size) < half
    c, s_ = cosine[...], sine[...]
    for s, out in enumerate(outs):
        at = pl.ds(pl.multiple_of((z ^ s) * both, both), both)
        for n, ref in enumerate((q, k)):
            x = ref[:, at].astype(jnp.float32)
            turned = jnp.where(front, pltpu.roll(x, both - half, 1), pltpu.roll(x, half, 1))
            out[n * rows : (n + 1) * rows, :] = (x * c + turned * s_).astype(jnp.bfloat16)
        out[2 * rows : 3 * rows, :] = v[:, at]


def attend_kernel(where, lam, gain, *refs, count, rows, size):
    own, other = refs[:count], refs[count]
    outs = refs[count + 1 : 2 * count + 1]
    qs, ks, vs, sems = refs[2 * count + 1 :]
    z, core = where[0], where[1]
    both = 2 * size
    value = vs.shape[1] // 2
    copies = []
    for s in range(count):
        mine = pl.multiple_of((2 * (z ^ s) + core) * rows, rows)
        theirs = pl.multiple_of((2 * (z ^ s) + 1 - core) * rows, rows)
        pairs = (
            (own[s].at[pl.ds(0, rows), :], qs.at[pl.ds(s * rows, rows), :]),
            (own[s].at[pl.ds(rows, rows), :], ks.at[pl.ds(mine, rows), :]),
            (own[s].at[pl.ds(2 * rows, rows), :], vs.at[pl.ds(mine, rows), pl.ds(0, value)]),
            (other.at[pl.ds(2 * s * rows, rows), :], ks.at[pl.ds(theirs, rows), :]),
            (
                other.at[pl.ds((2 * s + 1) * rows, rows), :],
                vs.at[pl.ds(theirs, rows), pl.ds(0, value)],
            ),
        )
        for n, (src, dst) in enumerate(pairs):
            copy = pltpu.make_async_copy(src, dst, sems.at[5 * s + n])
            copy.start()
            copies.append(copy)
    vs[:, value:] = jnp.ones((vs.shape[0], value), jnp.bfloat16)
    for copy in copies:
        copy.wait()
    factor = LOG2E * size ** (-0.5)
    lane = lax.broadcasted_iota(jnp.int32, (rows, both), 1)
    row_at = lax.broadcasted_iota(jnp.int32, (rows, rows), 0)
    col_at = lax.broadcasted_iota(jnp.int32, (rows, rows), 1)
    allowed = jnp.concatenate([col_at <= row_at] * 2, axis=0)
    zero = jnp.zeros((rows, both), jnp.bfloat16)
    contract = (((1,), (1,)), ((), ()))
    for s in range(count):
        q = qs[s * rows : (s + 1) * rows, :]
        stacked = jnp.concatenate(
            [jnp.where(lane < size, q, zero), jnp.where(lane < size, zero, q)], axis=0
        )
        last = 2 * (z ^ s) + core

        def step(block, current, diagonal):
            top, acc = current
            at = pl.ds(pl.multiple_of(block * rows, rows), rows)
            scores = (
                lax.dot_general(stacked, ks[at, :], contract, preferred_element_type=jnp.float32)
                * factor
            )
            if diagonal:
                scores = jnp.where(allowed, scores, masked_low)
            new_top = jnp.maximum(top, jnp.max(scores, axis=1, keepdims=True))
            weights = jnp.exp2(scores - new_top).astype(jnp.bfloat16)
            acc = acc * jnp.exp2(top - new_top) + jnp.dot(
                weights, vs[at, :], preferred_element_type=jnp.float32
            )
            return new_top, acc

        start = (
            jnp.full((2 * rows, 1), masked_low, jnp.float32),
            jnp.zeros((2 * rows, 2 * value), jnp.float32),
        )
        current = step(last, start, True)
        _, acc = lax.fori_loop(0, last, lambda n, cur: step(n, cur, False), current)
        maps = acc[:, :value] / acc[:, value:]
        diff = maps[:rows] - lam[z] * maps[rows:]
        inverse = lax.rsqrt(jnp.mean(diff * diff, axis=1, keepdims=True) + norm_eps)
        outs[s][...] = (diff * inverse * gain[...]).astype(jnp.bfloat16)


def project_kernel(where, *refs, count, tp):
    heads, weight, outs, rows_ref = refs[:count], refs[count], refs[count + 1 : -1], refs[-1]
    z, ti = where[0], where[2]
    value = heads[0].shape[1]
    for s in range(count):
        rows_ref[:, pl.ds(pl.multiple_of((z ^ s) * value, value), value)] = heads[s][...]
    rows = rows_ref[...]
    cols = outs[0].shape[1]
    for s in range(tp):
        at = pl.ds(pl.multiple_of((ti ^ s) * cols, cols), cols)
        outs[s][...] = jnp.dot(rows, weight[:, at], preferred_element_type=jnp.float32).astype(
            jnp.bfloat16
        )


def rotate(inputs, positions):
    half_size = inputs.shape[-1] // 2
    frequency = theta_base ** (-(jnp.arange(half_size, dtype=jnp.float32) * 2.0) / inputs.shape[-1])
    angles = positions.astype(jnp.float32)[:, None] * frequency[None, :]
    cosine = jnp.cos(angles)[:, None, None, :]
    sine_part = jnp.sin(angles)[:, None, None, :]
    front_half = inputs[..., :half_size]
    back_half = inputs[..., half_size:]
    return jnp.concatenate(
        [front_half * cosine - back_half * sine_part, back_half * cosine + front_half * sine_part],
        axis=-1,
    )


def gathered_attention(query_pairs, key_pairs, value_rows, head_lambda, head_gain):
    local_rows = query_pairs.shape[0]
    local_heads = head_lambda.shape[0]
    head_size = query_pairs.shape[1] // (2 * local_heads)
    value_size = value_rows.shape[1] // local_heads
    positions = lax.axis_index("ep") * local_rows + jnp.arange(local_rows, dtype=jnp.int32)
    rot_queries = rotate(
        query_pairs.astype(jnp.float32).reshape(local_rows, local_heads, 2, head_size), positions
    ).astype(jnp.bfloat16)
    rot_keys = rotate(
        key_pairs.astype(jnp.float32).reshape(local_rows, local_heads, 2, head_size), positions
    ).astype(jnp.bfloat16)
    rot_keys = rot_keys.reshape(local_rows, local_heads * 2 * head_size)
    zero_init = (
        jnp.full((local_heads, 2, local_rows), masked_low, jnp.float32),
        jnp.zeros((local_heads, 2, local_rows), jnp.float32),
        jnp.zeros((local_heads, 2, local_rows, value_size), jnp.float32),
    )
    piece_keys = lax.all_gather(rot_keys, "ep", axis=0, tiled=True)
    piece_values = lax.all_gather(value_rows, "ep", axis=0, tiled=True)
    block_count = piece_keys.shape[0] // KEY_BLOCK
    group_size = 4 if block_count % 4 == 0 else 1
    group_count = block_count // group_size
    grouped_keys = piece_keys.reshape(group_count, group_size, KEY_BLOCK, local_heads, 2, head_size)
    grouped_values = piece_values.reshape(
        group_count, group_size, KEY_BLOCK, local_heads, value_size
    )

    def one_group(current, inputs):
        block_keys, block_values, group_index = inputs
        key_positions = group_index * group_size * KEY_BLOCK + jnp.arange(
            group_size * KEY_BLOCK, dtype=jnp.int32
        ).reshape(group_size, KEY_BLOCK)
        scores = jnp.einsum(
            "qhmd,gkhmd->hmqgk", rot_queries, block_keys, preferred_element_type=jnp.float32
        ) * head_size ** (-0.5)
        allowed = key_positions[None, :, :] <= positions[:, None, None]
        scores = jnp.where(allowed, scores, masked_low)
        block_max = jnp.max(scores, axis=-1)
        weights = jnp.where(allowed, jnp.exp(scores - block_max[..., None]), 0.0)
        block_sum = jnp.sum(weights, axis=-1)
        block_out = jnp.einsum(
            "hmqgk,gkhc->hmqgc",
            weights.astype(jnp.bfloat16),
            block_values,
            preferred_element_type=jnp.float32,
        )
        run_max, run_sum, run_out = current
        new_max = jnp.maximum(run_max, jnp.max(block_max, axis=-1))
        old_scale = jnp.exp(run_max - new_max)
        new_scale = jnp.exp(block_max - new_max[..., None])
        run_sum = run_sum * old_scale + jnp.sum(new_scale * block_sum, axis=-1)
        run_out = run_out * old_scale[..., None] + jnp.sum(
            new_scale[..., None] * block_out, axis=-2
        )
        return ((new_max, run_sum, run_out), None)

    result, _ = lax.scan(
        one_group,
        zero_init,
        (grouped_keys, grouped_values, jnp.arange(group_count, dtype=jnp.int32)),
    )
    run_max, run_sum, run_out = result
    map_outputs = run_out / run_sum[..., None]
    difference = map_outputs[:, 0] - head_lambda[:, None, None] * map_outputs[:, 1]
    inverse_rms = lax.rsqrt(jnp.mean(difference * difference, axis=-1, keepdims=True) + norm_eps)
    normed_heads = (difference * inverse_rms * head_gain).astype(jnp.bfloat16)
    return [normed_heads.transpose(1, 0, 2).reshape(local_rows, local_heads * value_size)]


def local(
    query_pairs,
    key_pairs,
    value_rows,
    head_lambda,
    head_gain,
    out_weight,
    moe_input,
    ffn_gain,
    routes,
    route_weight,
    gate_weight,
    up_weight,
    down_weight,
    shared_gate,
    shared_up,
    shared_down,
):
    ep, tp = lax.axis_size("ep"), lax.axis_size("tp")
    chips = ep // 2
    ei, ti = lax.axis_index("ep"), lax.axis_index("tp")
    z, core = ei // 2, ei % 2
    where = jnp.stack([z, core, ti]).astype(jnp.int32)
    tx = ti.astype(jnp.int32)

    def along_z(x, s):
        return lax.ppermute(x, "ep", [(i, 2 * ((i // 2) ^ s) + i % 2) for i in range(ep)])

    def swap(x):
        return lax.ppermute(x, "ep", [(i, i ^ 1) for i in range(ep)])

    def along_tp(x, s):
        return lax.ppermute(x, "tp", [(i, i ^ s) for i in range(tp)])

    def exchange(parts, move):
        return [parts[0]] + [move(parts[s], s) for s in range(1, len(parts))]

    tokens, width = moe_input.shape
    cap = tokens * TOP_K * 5 // (4 * ep)
    slice_width = width // tp
    xn, slots, *parts = pl.pallas_call(
        lambda *refs: dispatch_kernel(*refs, cap=cap, experts=ep),
        out_shape=[sds((tokens, width)), sds((tokens, TOP_K), jnp.int32)]
        + [sds((2 * cap, slice_width))] * chips,
        in_specs=[SM] + [VM] * 4,
        out_specs=[VM] * (2 + chips),
        cost_estimate=cost(4e8),
        name="dispatch",
    )(where, moe_input, ffn_gain.reshape(1, -1), routes, routes.T)
    arrived = exchange(parts, along_z)

    rows = query_pairs.shape[0]
    heads = head_lambda.shape[0]
    size = query_pairs.shape[1] // (2 * heads)
    value = value_rows.shape[1] // heads
    spread = heads == chips and value == 2 * size and value % 128 == 0
    if spread:
        positions = (ei * rows + jnp.arange(rows, dtype=jnp.int32)).astype(jnp.float32)
        index = jnp.arange(2 * size, dtype=jnp.int32)
        frequency = theta_base ** (-((index % (size // 2)).astype(jnp.float32) * 2.0) / size)
        angles = positions[:, None] * frequency[None, :]
        sign = jnp.where(index % size < size // 2, -1.0, 1.0).astype(jnp.float32)
        cosine = jnp.cos(angles)
        sine = jnp.sin(angles) * sign
        packs = pl.pallas_call(
            lambda *refs: rope_kernel(*refs, size=size),
            out_shape=[sds((3 * rows, value))] * chips,
            in_specs=[SM] + [VM] * 5,
            out_specs=[VM] * chips,
            cost_estimate=cost(4e8),
            name="rope",
        )(where, query_pairs, key_pairs, value_rows, cosine, sine)
        packs = exchange(packs, along_z)
        other = swap(jnp.concatenate([p[rows:] for p in packs], axis=0))

    shared = run_expert(tx, [xn], shared_gate, shared_up, shared_down, tp, "shared_expert")
    shared = exchange(shared, along_tp)

    swapped = swap(jnp.concatenate([p[cap:] for p in arrived], axis=0))
    held = jnp.concatenate([p[:cap] for p in arrived] + [swapped], axis=0)
    slices = [held] + [along_tp(held, s) for s in range(1, tp)]
    terms = run_expert(tx, slices, gate_weight[0], up_weight[0], down_weight[0], tp, "routed_expert")
    terms = exchange(terms, along_tp)
    summed = sum(t.astype(jnp.float32) for t in terms).astype(jnp.bfloat16)

    if spread:
        heads_out = pl.pallas_call(
            lambda *refs: attend_kernel(*refs, count=chips, rows=rows, size=size),
            out_shape=[sds((rows, value))] * chips,
            in_specs=[SM, SM, VM] + [ANY] * (chips + 1),
            out_specs=[VM] * chips,
            scratch_shapes=[
                pltpu.VMEM((chips * rows, value), jnp.bfloat16),
                pltpu.VMEM((ep * rows, value), jnp.bfloat16),
                pltpu.VMEM((ep * rows, 2 * value), jnp.bfloat16),
                pltpu.SemaphoreType.DMA((5 * chips,)),
            ],
            cost_estimate=cost(4e9),
            name="attend",
        )(where, head_lambda, head_gain.reshape(1, -1), *packs, other)
        normed = exchange(heads_out, along_z)
        mixer = pl.pallas_call(
            lambda *refs: project_kernel(*refs, count=chips, tp=tp),
            out_shape=[sds((rows, out_weight.shape[1] // tp))] * tp,
            in_specs=[SM] + [VM] * (chips + 1),
            out_specs=[VM] * tp,
            scratch_shapes=[pltpu.VMEM((rows, chips * value), jnp.bfloat16)],
            cost_estimate=cost(1e9),
            name="project",
        )(where, *normed, out_weight)
        mixer = exchange(mixer, along_tp)
        attn_out = sum(m.astype(jnp.float32) for m in mixer).astype(jnp.bfloat16)
    else:
        head_rows = gathered_attention(query_pairs, key_pairs, value_rows, head_lambda, head_gain)[0]
        mixer = jnp.dot(head_rows, out_weight, preferred_element_type=jnp.float32)
        attn_out = lax.psum_scatter(
            mixer.astype(jnp.bfloat16), "tp", scatter_dimension=1, tiled=True
        )

    half = chips * cap
    back = swap(summed[half:])
    groups = [
        jnp.concatenate([summed[s * cap : (s + 1) * cap], back[s * cap : (s + 1) * cap]], axis=0)
        for s in range(chips)
    ]
    groups = exchange(groups, along_z)
    moe_out = pl.pallas_call(
        lambda *refs: combine_kernel(*refs, count=chips),
        out_shape=sds((tokens, slice_width)),
        in_specs=[VM] * (2 + chips + tp),
        out_specs=VM,
        cost_estimate=cost(4e8),
        name="combine",
    )(slots, route_weight, *groups, *shared)
    return (attn_out, moe_out)


def solution(mesh):
    return jax.shard_map(
        local,
        mesh=mesh,
        in_specs=(
            P("ep", "tp"),
            P("ep", "tp"),
            P("ep", "tp"),
            P("tp"),
            P(),
            P("tp", None),
            P("ep", None),
            P(),
            P("ep", None),
            P("ep", None),
            P("ep", None, "tp"),
            P("ep", None, "tp"),
            P("ep", "tp", None),
            P(None, "tp"),
            P(None, "tp"),
            P("tp", None),
        ),
        out_specs=(P("ep", "tp"), P("ep", "tp")),
        check_vma=False,
    )
```

```python
import math

import jax
import jax.numpy as jnp
from jax import lax
from jax.experimental import pallas as pl
from jax.experimental.pallas import tpu as pltpu
from jax.sharding import PartitionSpec as P


TOP_K = 2
KEY_BLOCK = 128

theta_base = 500000.0
norm_eps = 1e-06
masked_low = -1e30
LOG2E = 1.4426950408889634

VM = pl.BlockSpec(memory_space=pltpu.VMEM)
SM = pl.BlockSpec(memory_space=pltpu.SMEM)
ANY = pl.BlockSpec(memory_space=pl.ANY)


def sds(shape, dtype=jnp.bfloat16):
    return jax.ShapeDtypeStruct(shape, dtype)


def limit(mib):
    return pltpu.CompilerParams(vmem_limit_bytes=mib * 1024 * 1024)


def cost(flops):
    return pl.CostEstimate(flops=int(flops), bytes_accessed=0, transcendentals=0)


def place():
    ei = lax.axis_index("ep")
    return ei // 2, ei % 2, lax.axis_index("tp")


def column(row):
    n = row.shape[1]
    at = lax.broadcasted_iota(jnp.int32, (n, n), 0)
    diagonal = at == lax.broadcasted_iota(jnp.int32, (n, n), 1)
    return jnp.sum(jnp.where(diagonal, row, jnp.zeros_like(row)), axis=1, keepdims=True)


def dispatch_kernel(rows, gain, routes, xn_out, slots_out, *parts, cap, experts):
    z, core, ti = place()
    tokens = rows.shape[0]
    values = rows[...].astype(jnp.float32)
    inverse = lax.rsqrt(jnp.mean(values * values, axis=-1, keepdims=True) + norm_eps)
    xn_out[...] = (values * inverse * gain[...]).astype(jnp.bfloat16)
    group = 2 * cap
    t_row = lax.broadcasted_iota(jnp.int32, (tokens, tokens), 0)
    t_col = lax.broadcasted_iota(jnp.int32, (tokens, tokens), 1)
    e_row = lax.broadcasted_iota(jnp.int32, (experts, tokens), 0)
    before = (t_row < t_col).astype(jnp.float32).astype(jnp.bfloat16)
    hits = [(e_row == routes[k : k + 1, :]).astype(jnp.float32) for k in range(TOP_K)]
    count = jnp.dot(sum(hits).astype(jnp.bfloat16), before, preferred_element_type=jnp.float32)
    slots = []
    for k in range(TOP_K):
        expert = routes[k : k + 1, :]
        rank = jnp.sum(count * hits[k], axis=0, keepdims=True).astype(jnp.int32)
        slots.append(((expert // 2) ^ z) * group + ((expert % 2) ^ core) * cap + rank)
        slots_out[k : k + 1, :] = slots[k]
    width = parts[0].shape[1]
    mine = xn_out[:, pl.ds(pl.multiple_of(ti * width, width), width)]
    for s, part in enumerate(parts):
        slot_row = lax.broadcasted_iota(jnp.int32, (group, tokens), 0) + s * group
        pick = slot_row == slots[0]
        for k in range(1, TOP_K):
            pick = pick | (slot_row == slots[k])
        pick = pick.astype(jnp.float32).astype(jnp.bfloat16)
        part[...] = jnp.dot(pick, mine, preferred_element_type=jnp.float32).astype(jnp.bfloat16)


def expert_kernel(*refs, pieces, outs):
    ti = place()[2]
    xs, (gate_w, up_w, down_w), ys = refs[:pieces], refs[pieces : pieces + 3], refs[pieces + 3 :]
    width = xs[0].shape[1]
    gate = up = None
    for s in range(pieces):
        if pieces == 1:
            wg, wu = gate_w[...], up_w[...]
        else:
            at = pl.ds(pl.multiple_of((ti ^ s) * width, width), width)
            wg, wu = gate_w[at, :], up_w[at, :]
        x = xs[s][...]
        g = jnp.dot(x, wg, preferred_element_type=jnp.float32)
        u = jnp.dot(x, wu, preferred_element_type=jnp.float32)
        gate = g if gate is None else gate + g
        up = u if up is None else up + u
    hidden = (gate / (1.0 + jnp.exp(-gate)) * up).astype(jnp.bfloat16)
    cols = ys[0].shape[1]
    for s in range(outs):
        at = pl.ds(pl.multiple_of((ti ^ s) * cols, cols), cols)
        ys[s][...] = jnp.dot(hidden, down_w[:, at], preferred_element_type=jnp.float32).astype(
            jnp.bfloat16
        )


def run_expert(xs, gate_w, up_w, down_w, tp):
    rows = xs[0].shape[0]
    width, hidden = gate_w.shape
    cols = down_w.shape[1] // tp
    return pl.pallas_call(
        lambda *refs: expert_kernel(*refs, pieces=len(xs), outs=tp),
        out_shape=[sds((rows, cols))] * tp,
        in_specs=[VM] * (len(xs) + 3),
        out_specs=[VM] * tp,
        cost_estimate=cost(6 * rows * width * hidden),
        compiler_params=limit(24),
    )(*xs, gate_w, up_w, down_w)


def combine_kernel(slots, weights, *refs, count):
    back, shared, out = refs[:count], refs[count:-1], refs[-1]
    tokens = slots.shape[1]
    own = [column(slots[k : k + 1, :]) for k in range(TOP_K)]
    scale = [column(weights[k : k + 1, :]) for k in range(TOP_K)]
    group = back[0].shape[0]
    total = None
    for part in shared:
        part = part[...].astype(jnp.float32)
        total = part if total is None else total + part
    picked = [None] * TOP_K
    for s in range(count):
        slot_col = lax.broadcasted_iota(jnp.int32, (tokens, group), 1) + s * group
        rows = back[s][...]
        for k in range(TOP_K):
            pick = (slot_col == own[k]).astype(jnp.float32).astype(jnp.bfloat16)
            term = jnp.dot(pick, rows, preferred_element_type=jnp.float32)
            picked[k] = term if picked[k] is None else picked[k] + term
    routed = scale[0] * picked[0]
    for k in range(1, TOP_K):
        routed = routed + scale[k] * picked[k]
    out[...] = (routed + total).astype(jnp.bfloat16)


def rope_kernel(q, k, v, cosine, sine, *outs, size):
    z = place()[0]
    rows = q.shape[0]
    both = cosine.shape[1]
    half = size // 2
    lane = lax.broadcasted_iota(jnp.int32, (rows, both), 1)
    front = (lane % size) < half
    c, s_ = cosine[...], sine[...]
    for s, out in enumerate(outs):
        at = pl.ds(pl.multiple_of((z ^ s) * both, both), both)
        for n, ref in enumerate((q, k)):
            x = ref[:, at].astype(jnp.float32)
            turned = jnp.where(front, pltpu.roll(x, both - half, 1), pltpu.roll(x, half, 1))
            out[n * rows : (n + 1) * rows, :] = (x * c + turned * s_).astype(jnp.bfloat16)
        out[2 * rows : 3 * rows, :] = v[:, at]


def attend_kernel(lam, gain, *refs, count, rows, size):
    own, other = refs[:count], refs[count]
    outs = refs[count + 1 : 2 * count + 1]
    qs, ks, vs, scores, weights, heads, sems = refs[2 * count + 1 :]
    z, core, _ = place()
    both = 2 * size
    value = vs.shape[1] // 2
    keys = 2 * rows
    copies = []
    for s in range(count):
        at = pl.multiple_of((z ^ s) * rows, rows)
        mine = pl.multiple_of((2 * (z ^ s) + core) * rows, rows)
        theirs = pl.multiple_of((2 * (z ^ s) + 1 - core) * rows, rows)
        pairs = (
            (own[s].at[pl.ds(0, rows), :], qs.at[pl.ds(at, rows), :]),
            (own[s].at[pl.ds(rows, rows), :], ks.at[pl.ds(mine, rows), :]),
            (own[s].at[pl.ds(2 * rows, rows), :], vs.at[pl.ds(mine, rows), pl.ds(0, value)]),
            (other.at[pl.ds(2 * s * rows, rows), :], ks.at[pl.ds(theirs, rows), :]),
            (
                other.at[pl.ds((2 * s + 1) * rows, rows), :],
                vs.at[pl.ds(theirs, rows), pl.ds(0, value)],
            ),
        )
        for n, (src, dst) in enumerate(pairs):
            copy = pltpu.make_async_copy(src, dst, sems.at[5 * s + n])
            copy.start()
            copies.append(copy)
    vs[:, value:] = jnp.ones((vs.shape[0], value), jnp.bfloat16)
    for copy in copies:
        copy.wait()
    factor = LOG2E * size ** (-0.5)
    lane = lax.broadcasted_iota(jnp.int32, (rows, both), 1)
    tile = math.gcd(rows, 64)
    ahead = lax.broadcasted_iota(jnp.int32, (tile, keys), 1) - lax.broadcasted_iota(
        jnp.int32, (tile, keys), 0
    )
    contract = (((1,), (1,)), ((), ()))
    units = [(block, m) for block in reversed(range(count)) for m in range(2)]
    maps = {}

    def score(u):
        block, m = units[u]
        q = qs[block * rows : (block + 1) * rows, :]
        q = jnp.where((lane < size) == (m == 0), q, jnp.zeros_like(q))
        for j in range(block + 1):
            at = slice(j * keys, (j + 1) * keys)
            scores[u % 2, :, at] = lax.dot_general(
                q, ks[at, :], contract, preferred_element_type=jnp.float32
            )

    def weigh(u):
        block, _ = units[u]
        for r in range(0, rows, tile):
            pieces = []
            for j in range(block + 1):
                piece = scores[u % 2, r : r + tile, j * keys : (j + 1) * keys]
                if j == block:
                    piece = jnp.where(ahead <= core * rows + r, piece, masked_low)
                pieces.append(piece)
            top = None
            for piece in pieces:
                one = jnp.max(piece, axis=1, keepdims=True)
                top = one if top is None else jnp.maximum(top, one)
            for j, piece in enumerate(pieces):
                weights[u % 2, r : r + tile, j * keys : (j + 1) * keys] = jnp.exp2(
                    (piece - top) * factor
                ).astype(jnp.bfloat16)

    def mix(u):
        block, m = units[u]
        span = (block + 1) * keys
        acc = jnp.dot(weights[u % 2, :, :span], vs[:span, :], preferred_element_type=jnp.float32)
        maps[m] = acc[:, :value] / acc[:, value:]
        if m == 1:
            diff = maps[0] - lam[z] * maps[1]
            inverse = lax.rsqrt(jnp.mean(diff * diff, axis=1, keepdims=True) + norm_eps)
            heads[block * rows : (block + 1) * rows, :] = (diff * inverse * gain[...]).astype(
                jnp.bfloat16
            )

    score(0)
    for u in range(len(units)):
        if u + 1 < len(units):
            score(u + 1)
        if u > 0:
            mix(u - 1)
        weigh(u)
    mix(len(units) - 1)
    for s in range(count):
        outs[s][...] = heads[pl.ds(pl.multiple_of((z ^ s) * rows, rows), rows), :]


def project_kernel(*refs, count, tp):
    heads, weight, outs, rows_ref = refs[:count], refs[count], refs[count + 1 : -1], refs[-1]
    z, _, ti = place()
    value = heads[0].shape[1]
    for s in range(count):
        rows_ref[:, pl.ds(pl.multiple_of((z ^ s) * value, value), value)] = heads[s][...]
    rows = rows_ref[...]
    cols = outs[0].shape[1]
    for s in range(tp):
        at = pl.ds(pl.multiple_of((ti ^ s) * cols, cols), cols)
        outs[s][...] = jnp.dot(rows, weight[:, at], preferred_element_type=jnp.float32).astype(
            jnp.bfloat16
        )


def rotate(inputs, positions):
    half_size = inputs.shape[-1] // 2
    frequency = theta_base ** (-(jnp.arange(half_size, dtype=jnp.float32) * 2.0) / inputs.shape[-1])
    angles = positions.astype(jnp.float32)[:, None] * frequency[None, :]
    cosine = jnp.cos(angles)[:, None, None, :]
    sine_part = jnp.sin(angles)[:, None, None, :]
    front_half = inputs[..., :half_size]
    back_half = inputs[..., half_size:]
    return jnp.concatenate(
        [front_half * cosine - back_half * sine_part, back_half * cosine + front_half * sine_part],
        axis=-1,
    )


def gathered_attention(query_pairs, key_pairs, value_rows, head_lambda, head_gain):
    local_rows = query_pairs.shape[0]
    local_heads = head_lambda.shape[0]
    head_size = query_pairs.shape[1] // (2 * local_heads)
    value_size = value_rows.shape[1] // local_heads
    positions = lax.axis_index("ep") * local_rows + jnp.arange(local_rows, dtype=jnp.int32)
    rot_queries = rotate(
        query_pairs.astype(jnp.float32).reshape(local_rows, local_heads, 2, head_size), positions
    ).astype(jnp.bfloat16)
    rot_keys = rotate(
        key_pairs.astype(jnp.float32).reshape(local_rows, local_heads, 2, head_size), positions
    ).astype(jnp.bfloat16)
    rot_keys = rot_keys.reshape(local_rows, local_heads * 2 * head_size)
    zero_init = (
        jnp.full((local_heads, 2, local_rows), masked_low, jnp.float32),
        jnp.zeros((local_heads, 2, local_rows), jnp.float32),
        jnp.zeros((local_heads, 2, local_rows, value_size), jnp.float32),
    )
    piece_keys = lax.all_gather(rot_keys, "ep", axis=0, tiled=True)
    piece_values = lax.all_gather(value_rows, "ep", axis=0, tiled=True)
    block_count = piece_keys.shape[0] // KEY_BLOCK
    group_size = 4 if block_count % 4 == 0 else 1
    group_count = block_count // group_size
    grouped_keys = piece_keys.reshape(group_count, group_size, KEY_BLOCK, local_heads, 2, head_size)
    grouped_values = piece_values.reshape(
        group_count, group_size, KEY_BLOCK, local_heads, value_size
    )

    def one_group(current, inputs):
        block_keys, block_values, group_index = inputs
        key_positions = group_index * group_size * KEY_BLOCK + jnp.arange(
            group_size * KEY_BLOCK, dtype=jnp.int32
        ).reshape(group_size, KEY_BLOCK)
        scores = jnp.einsum(
            "qhmd,gkhmd->hmqgk", rot_queries, block_keys, preferred_element_type=jnp.float32
        ) * head_size ** (-0.5)
        allowed = key_positions[None, :, :] <= positions[:, None, None]
        scores = jnp.where(allowed, scores, masked_low)
        block_max = jnp.max(scores, axis=-1)
        weights = jnp.where(allowed, jnp.exp(scores - block_max[..., None]), 0.0)
        block_sum = jnp.sum(weights, axis=-1)
        block_out = jnp.einsum(
            "hmqgk,gkhc->hmqgc",
            weights.astype(jnp.bfloat16),
            block_values,
            preferred_element_type=jnp.float32,
        )
        run_max, run_sum, run_out = current
        new_max = jnp.maximum(run_max, jnp.max(block_max, axis=-1))
        old_scale = jnp.exp(run_max - new_max)
        new_scale = jnp.exp(block_max - new_max[..., None])
        run_sum = run_sum * old_scale + jnp.sum(new_scale * block_sum, axis=-1)
        run_out = run_out * old_scale[..., None] + jnp.sum(
            new_scale[..., None] * block_out, axis=-2
        )
        return ((new_max, run_sum, run_out), None)

    result, _ = lax.scan(
        one_group,
        zero_init,
        (grouped_keys, grouped_values, jnp.arange(group_count, dtype=jnp.int32)),
    )
    _, run_sum, run_out = result
    map_outputs = run_out / run_sum[..., None]
    difference = map_outputs[:, 0] - head_lambda[:, None, None] * map_outputs[:, 1]
    inverse_rms = lax.rsqrt(jnp.mean(difference * difference, axis=-1, keepdims=True) + norm_eps)
    normed_heads = (difference * inverse_rms * head_gain).astype(jnp.bfloat16)
    return [normed_heads.transpose(1, 0, 2).reshape(local_rows, local_heads * value_size)]


def inner(
    query_pairs,
    key_pairs,
    value_rows,
    head_lambda,
    head_gain,
    out_weight,
    moe_input,
    ffn_gain,
    routes,
    route_weight,
    gate_weight,
    up_weight,
    down_weight,
    shared_gate,
    shared_up,
    shared_down,
):
    ep, tp = lax.axis_size("ep"), lax.axis_size("tp")
    chips = ep // 2
    ei = lax.axis_index("ep")

    def along_z(x, s):
        return lax.ppermute(x, "ep", [(i, 2 * ((i // 2) ^ s) + i % 2) for i in range(ep)])

    def swap(x):
        return lax.ppermute(x, "ep", [(i, i ^ 1) for i in range(ep)])

    def along_tp(x, s):
        return lax.ppermute(x, "tp", [(i, i ^ s) for i in range(tp)])

    def exchange(parts, move):
        return [parts[0]] + [move(parts[s], s) for s in range(1, len(parts))]

    tokens, width = moe_input.shape
    cap = tokens * TOP_K * 5 // (4 * ep)
    slice_width = width // tp
    xn, slots, *parts = pl.pallas_call(
        lambda *refs: dispatch_kernel(*refs, cap=cap, experts=ep),
        out_shape=[sds((tokens, width)), sds((TOP_K, tokens), jnp.int32)]
        + [sds((2 * cap, slice_width))] * chips,
        in_specs=[VM] * 3,
        out_specs=[VM] * (2 + chips),
        cost_estimate=cost(4e8),
        name="dispatch",
        compiler_params=limit(8),
    )(moe_input, ffn_gain.reshape(1, -1), routes.T)
    arrived = exchange(parts, along_z)

    rows = query_pairs.shape[0]
    heads = head_lambda.shape[0]
    size = query_pairs.shape[1] // (2 * heads)
    value = value_rows.shape[1] // heads
    spread = heads == chips and value == 2 * size and value % 128 == 0
    if spread:
        positions = (ei * rows + jnp.arange(rows, dtype=jnp.int32)).astype(jnp.float32)
        index = jnp.arange(2 * size, dtype=jnp.int32)
        frequency = theta_base ** (-((index % (size // 2)).astype(jnp.float32) * 2.0) / size)
        angles = positions[:, None] * frequency[None, :]
        sign = jnp.where(index % size < size // 2, -1.0, 1.0).astype(jnp.float32)
        cosine = jnp.cos(angles)
        sine = jnp.sin(angles) * sign
        packs = pl.pallas_call(
            lambda *refs: rope_kernel(*refs, size=size),
            out_shape=[sds((3 * rows, value))] * chips,
            in_specs=[VM] * 5,
            out_specs=[VM] * chips,
            cost_estimate=cost(4e8),
            name="rope",
        compiler_params=limit(8),
        )(query_pairs, key_pairs, value_rows, cosine, sine)
        packs = exchange(packs, along_z)
        other = jnp.concatenate([p[rows:] for p in packs], axis=0)
        other = swap(other)

    shared = run_expert([xn], shared_gate, shared_up, shared_down, tp)
    shared = exchange(shared, along_tp)

    swapped = swap(jnp.concatenate([p[cap:] for p in arrived], axis=0))
    held = jnp.concatenate([p[:cap] for p in arrived] + [swapped], axis=0)
    slices = [held] + [along_tp(held, s) for s in range(1, tp)]
    terms = run_expert(slices, gate_weight[0], up_weight[0], down_weight[0], tp)
    terms = exchange(terms, along_tp)
    summed = sum(t.astype(jnp.float32) for t in terms).astype(jnp.bfloat16)

    if spread:
        heads_out = pl.pallas_call(
            lambda *refs: attend_kernel(*refs, count=chips, rows=rows, size=size),
            out_shape=[sds((rows, value))] * chips,
            in_specs=[SM, VM] + [ANY] * (chips + 1),
            out_specs=[VM] * chips,
            scratch_shapes=[
                pltpu.VMEM((chips * rows, value), jnp.bfloat16),
                pltpu.VMEM((ep * rows, value), jnp.bfloat16),
                pltpu.VMEM((ep * rows, 2 * value), jnp.bfloat16),
                pltpu.VMEM((2, rows, ep * rows), jnp.float32),
                pltpu.VMEM((2, rows, ep * rows), jnp.bfloat16),
                pltpu.VMEM((chips * rows, value), jnp.bfloat16),
                pltpu.SemaphoreType.DMA((5 * chips,)),
            ],
            cost_estimate=cost(4e9),
            name="attend",
        compiler_params=limit(32),
        )(head_lambda, head_gain.reshape(1, -1), *packs, other)
        normed = exchange(heads_out, along_z)
        mixer = pl.pallas_call(
            lambda *refs: project_kernel(*refs, count=chips, tp=tp),
            out_shape=[sds((rows, out_weight.shape[1] // tp))] * tp,
            in_specs=[VM] * (chips + 1),
            out_specs=[VM] * tp,
            scratch_shapes=[pltpu.VMEM((rows, chips * value), jnp.bfloat16)],
            cost_estimate=cost(1e9),
            name="project",
        compiler_params=limit(10),
        )(*normed, out_weight)
        mixer = exchange(mixer, along_tp)
        attn_out = sum(m.astype(jnp.float32) for m in mixer).astype(jnp.bfloat16)
    else:
        head_rows = gathered_attention(query_pairs, key_pairs, value_rows, head_lambda, head_gain)[0]
        mixer = jnp.dot(head_rows, out_weight, preferred_element_type=jnp.float32)
        attn_out = lax.psum_scatter(
            mixer.astype(jnp.bfloat16), "tp", scatter_dimension=1, tiled=True
        )

    half = chips * cap
    back = swap(summed[half:])
    groups = [
        jnp.concatenate([summed[s * cap : (s + 1) * cap], back[s * cap : (s + 1) * cap]], axis=0)
        for s in range(chips)
    ]
    groups = exchange(groups, along_z)
    moe_out = pl.pallas_call(
        lambda *refs: combine_kernel(*refs, count=chips),
        out_shape=sds((tokens, slice_width)),
        in_specs=[VM] * (2 + chips + tp),
        out_specs=VM,
        cost_estimate=cost(4e8),
        name="combine",
        compiler_params=limit(10),
    )(slots, route_weight.T, *groups, *shared)
    return (attn_out, moe_out)


def solution(mesh):
    return jax.shard_map(
        inner,
        mesh=mesh,
        in_specs=(
            P("ep", "tp"),
            P("ep", "tp"),
            P("ep", "tp"),
            P("tp"),
            P(),
            P("tp", None),
            P("ep", None),
            P(),
            P("ep", None),
            P("ep", None),
            P("ep", None, "tp"),
            P("ep", None, "tp"),
            P("ep", "tp", None),
            P(None, "tp"),
            P(None, "tp"),
            P("tp", None),
        ),
        out_specs=(P("ep", "tp"), P("ep", "tp")),
        check_vma=False,
    )
```

```python
import math

import jax
import jax.numpy as jnp
from jax import lax
from jax.experimental import pallas as pl
from jax.experimental.pallas import tpu as pltpu
from jax.sharding import PartitionSpec as P


TOP_K = 2
KEY_BLOCK = 128

theta_base = 500000.0
norm_eps = 1e-06
masked_low = -1e30
LOG2E = 1.4426950408889634

VM = pl.BlockSpec(memory_space=pltpu.VMEM)
SM = pl.BlockSpec(memory_space=pltpu.SMEM)
ANY = pl.BlockSpec(memory_space=pl.ANY)
FAR = pl.BlockSpec(memory_space=pltpu.HBM)
DMA = pltpu.SemaphoreType.DMA


def sds(shape, dtype=jnp.bfloat16):
    return jax.ShapeDtypeStruct(shape, dtype)


def limit(mib):
    return pltpu.CompilerParams(vmem_limit_bytes=mib * 1024 * 1024)


def far(x):
    return pltpu.with_memory_space_constraint(x, pltpu.HBM)


def begin(pairs, sems):
    copies = [pltpu.make_async_copy(a, b, sems.at[n]) for n, (a, b) in enumerate(pairs)]
    for copy in copies:
        copy.start()
    return copies


def cost(flops):
    return pl.CostEstimate(flops=int(flops), bytes_accessed=0, transcendentals=0)


def place():
    ei = lax.axis_index("ep")
    return ei // 2, ei % 2, lax.axis_index("tp")


def column(row):
    n = row.shape[1]
    at = lax.broadcasted_iota(jnp.int32, (n, n), 0)
    diagonal = at == lax.broadcasted_iota(jnp.int32, (n, n), 1)
    return jnp.sum(jnp.where(diagonal, row, jnp.zeros_like(row)), axis=1, keepdims=True)


def dispatch_kernel(rows_far, gain_far, routes_far, xn_out, slots_out, *refs, cap, experts):
    *parts, rows, gain, routes, sems = refs
    z, core, ti = place()
    tokens = rows.shape[0]
    for copy in begin(((rows_far, rows), (gain_far, gain), (routes_far, routes)), sems):
        copy.wait()
    values = rows[...].astype(jnp.float32)
    inverse = lax.rsqrt(jnp.mean(values * values, axis=-1, keepdims=True) + norm_eps)
    xn_out[...] = (values * inverse * gain[...]).astype(jnp.bfloat16)
    group = 2 * cap
    t_row = lax.broadcasted_iota(jnp.int32, (tokens, tokens), 0)
    t_col = lax.broadcasted_iota(jnp.int32, (tokens, tokens), 1)
    e_row = lax.broadcasted_iota(jnp.int32, (experts, tokens), 0)
    before = (t_row < t_col).astype(jnp.float32).astype(jnp.bfloat16)
    hits = [(e_row == routes[k : k + 1, :]).astype(jnp.float32) for k in range(TOP_K)]
    count = jnp.dot(sum(hits).astype(jnp.bfloat16), before, preferred_element_type=jnp.float32)
    slots = []
    for k in range(TOP_K):
        expert = routes[k : k + 1, :]
        rank = jnp.sum(count * hits[k], axis=0, keepdims=True).astype(jnp.int32)
        slots.append(((expert // 2) ^ z) * group + ((expert % 2) ^ core) * cap + rank)
        slots_out[k : k + 1, :] = slots[k]
    width = parts[0].shape[1]
    mine = xn_out[:, pl.ds(pl.multiple_of(ti * width, width), width)]
    for s, part in enumerate(parts):
        slot_row = lax.broadcasted_iota(jnp.int32, (group, tokens), 0) + s * group
        pick = slot_row == slots[0]
        for k in range(1, TOP_K):
            pick = pick | (slot_row == slots[k])
        pick = pick.astype(jnp.float32).astype(jnp.bfloat16)
        part[...] = jnp.dot(pick, mine, preferred_element_type=jnp.float32).astype(jnp.bfloat16)


def pack_kernel(*refs, count, cap):
    parts, own, other = refs[:count], refs[count], refs[count + 1]
    for s in range(count):
        own[s * cap : (s + 1) * cap, :] = parts[s][:cap, :]
        other[s * cap : (s + 1) * cap, :] = parts[s][cap:, :]


def spread_out(block, ti, outs, direct):
    if direct:
        for s, out in enumerate(outs):
            out[...] = block(ti ^ s).astype(jnp.bfloat16)
        return
    send_x, keep_x, send_y, keep_y = outs
    half = send_x.shape[0] // 2
    for s, upper, lower in ((0, (keep_x, 0), (keep_y, 0)), (1, (send_x, 0), (keep_y, half)),
                            (2, (keep_x, half), (send_y, 0)), (3, (send_x, half), (send_y, half))):
        values = block(ti ^ s).astype(jnp.bfloat16)
        for (ref, at), piece in ((upper, values[:half]), (lower, values[half:])):
            ref[at : at + half, :] = piece


def expert_kernel(*refs, pieces, halves, direct, staged):
    ti = place()[2]
    xs, (gate_w, up_w, down_w) = refs[: pieces * halves], refs[pieces * halves :][:3]
    rest = refs[pieces * halves + 3 :]
    chunks = pieces
    if staged:
        *ys, rows_ref, gates, ups, downs, sems = rest
        chunks = gates.shape[0]
        width = gates.shape[1]
        pairs = []
        for s in range(chunks):
            at = pl.ds(pl.multiple_of((ti ^ s) * width, width), width)
            pairs += [(gate_w.at[at, :], gates.at[s]), (up_w.at[at, :], ups.at[s])]
        copies = begin(pairs + [(down_w, downs)], sems)
    else:
        *ys, rows_ref = rest
        width = gate_w.shape[0] // chunks
        downs = down_w
    gate = up = None
    for s in range(chunks):
        part = xs[0].shape[0]
        at = pl.ds(pl.multiple_of((ti ^ s) * width, width), width)
        if pieces == 1:
            x = xs[0][:, at]
        else:
            for h in range(halves):
                rows_ref[s % 2, h * part : (h + 1) * part, :] = xs[h * pieces + s][...]
            x = rows_ref[s % 2]
        if staged:
            copies[2 * s].wait()
            copies[2 * s + 1].wait()
            wg, wu = gates[s], ups[s]
        else:
            wg, wu = gate_w[at, :], up_w[at, :]
        g = jnp.dot(x, wg, preferred_element_type=jnp.float32)
        u = jnp.dot(x, wu, preferred_element_type=jnp.float32)
        gate = g if gate is None else gate + g
        up = u if up is None else up + u
    hidden = (gate / (1.0 + jnp.exp(-gate)) * up).astype(jnp.bfloat16)
    if staged:
        copies[-1].wait()
    cols = ys[0].shape[1]

    def block(n):
        at = pl.ds(pl.multiple_of(n * cols, cols), cols)
        return jnp.dot(hidden, downs[:, at], preferred_element_type=jnp.float32)

    spread_out(block, ti, ys, direct)


def out_shapes(rows, cols, tp, direct):
    return [sds((rows, cols))] * (tp if direct else 4)


def run_expert(xs, halves, gate_w, up_w, down_w, tp, direct):
    rows = xs[0].shape[0] * halves
    width, hidden = gate_w.shape
    shapes = out_shapes(rows, down_w.shape[1] // tp, tp, direct)
    pieces = len(xs) // halves
    staged = pieces == 1
    scratch = [pltpu.VMEM((2, rows, width // tp), jnp.bfloat16)]
    if staged:
        part = pltpu.VMEM((tp, width // tp, hidden), jnp.bfloat16)
        scratch += [part, part, pltpu.VMEM(down_w.shape, jnp.bfloat16), DMA((2 * tp + 1,))]
        gate_w, up_w, down_w = far(gate_w), far(up_w), far(down_w)
    return pl.pallas_call(
        lambda *refs: expert_kernel(*refs, pieces=pieces, halves=halves, direct=direct, staged=staged),
        out_shape=shapes,
        in_specs=[VM] * len(xs) + [FAR if staged else VM] * 3,
        out_specs=[VM] * len(shapes),
        scratch_shapes=scratch,
        cost_estimate=cost(6 * rows * width * hidden),
        compiler_params=limit(24),
    )(*xs, gate_w, up_w, down_w)


def combine_kernel(slots, weights, *refs, count):
    back, shared, out = refs[:count], refs[count:-1], refs[-1]
    tokens = slots.shape[1]
    own = [column(slots[k : k + 1, :]) for k in range(TOP_K)]
    scale = [column(weights[k : k + 1, :]) for k in range(TOP_K)]
    group = back[0].shape[0]
    total = None
    for part in shared:
        part = part[...].astype(jnp.float32)
        total = part if total is None else total + part
    picked = [None] * TOP_K
    for s in range(count):
        slot_col = lax.broadcasted_iota(jnp.int32, (tokens, group), 1) + s * group
        rows = back[s][...]
        for k in range(TOP_K):
            pick = (slot_col == own[k]).astype(jnp.float32).astype(jnp.bfloat16)
            term = jnp.dot(pick, rows, preferred_element_type=jnp.float32)
            picked[k] = term if picked[k] is None else picked[k] + term
    routed = scale[0] * picked[0]
    for k in range(1, TOP_K):
        routed = routed + scale[k] * picked[k]
    out[...] = (routed + total).astype(jnp.bfloat16)


def rope_kernel(q_far, k_far, v_far, cosine, sine, *refs, size):
    *outs, q, k, v, sems = refs
    copies = begin(((q_far, q), (k_far, k), (v_far, v)), sems)
    z = place()[0]
    rows = q.shape[0]
    both = cosine.shape[1]
    half = size // 2
    lane = lax.broadcasted_iota(jnp.int32, (rows, both), 1)
    front = (lane % size) < half
    c, s_ = cosine[...], sine[...]
    for copy in copies:
        copy.wait()
    for s, out in enumerate(outs):
        at = pl.ds(pl.multiple_of((z ^ s) * both, both), both)
        for n, ref in enumerate((q, k)):
            x = ref[:, at].astype(jnp.float32)
            turned = jnp.where(front, pltpu.roll(x, both - half, 1), pltpu.roll(x, half, 1))
            out[n * rows : (n + 1) * rows, :] = (x * c + turned * s_).astype(jnp.bfloat16)
        out[2 * rows : 3 * rows, :] = v[:, at]


def attend_kernel(lam_far, gain_far, *refs, count, rows, size):
    own, other, outs = refs[:count], refs[count : 2 * count], refs[2 * count : 3 * count]
    qs, ks, vs, scores, weights, heads, lam, gain, sems = refs[3 * count :]
    z, core, _ = place()
    both = 2 * size
    value = vs.shape[1] // 2
    keys = 2 * rows
    pairs = [(lam_far, lam), (gain_far, gain)]
    for s in range(count):
        at = pl.multiple_of((z ^ s) * rows, rows)
        mine = pl.multiple_of((2 * (z ^ s) + core) * rows, rows)
        theirs = pl.multiple_of((2 * (z ^ s) + 1 - core) * rows, rows)
        pairs.append((own[s].at[pl.ds(0, rows), :], qs.at[pl.ds(at, rows), :]))
        for ref, to in ((own[s], mine), (other[s], theirs)):
            k_rows, v_rows, to = pl.ds(rows, rows), pl.ds(2 * rows, rows), pl.ds(to, rows)
            pairs.append((ref.at[k_rows, :], ks.at[to, :]))
            pairs.append((ref.at[v_rows, :], vs.at[to, pl.ds(0, value)]))
    copies = begin(pairs, sems)
    vs[:, value:] = jnp.ones((vs.shape[0], value), jnp.bfloat16)
    for copy in copies:
        copy.wait()
    factor = LOG2E * size ** (-0.5)
    lane = lax.broadcasted_iota(jnp.int32, (rows, both), 1)
    tile = math.gcd(rows, 64)
    ahead = lax.broadcasted_iota(jnp.int32, (tile, keys), 1) - lax.broadcasted_iota(
        jnp.int32, (tile, keys), 0
    )
    contract = (((1,), (1,)), ((), ()))
    units = [(block, m) for block in reversed(range(count)) for m in range(2)]
    maps = {}

    def score(u):
        block, m = units[u]
        q = qs[block * rows : (block + 1) * rows, :]
        q = jnp.where((lane < size) == (m == 0), q, jnp.zeros_like(q))
        for j in range(block + 1):
            at = slice(j * keys, (j + 1) * keys)
            scores[u % 2, :, at] = lax.dot_general(
                q, ks[at, :], contract, preferred_element_type=jnp.float32
            )

    def weigh(u):
        block, _ = units[u]
        for r in range(0, rows, tile):
            pieces = []
            for j in range(block + 1):
                piece = scores[u % 2, r : r + tile, j * keys : (j + 1) * keys]
                if j == block:
                    piece = jnp.where(ahead <= core * rows + r, piece, masked_low)
                pieces.append(piece)
            top = None
            for piece in pieces:
                one = jnp.max(piece, axis=1, keepdims=True)
                top = one if top is None else jnp.maximum(top, one)
            for j, piece in enumerate(pieces):
                weights[u % 2, r : r + tile, j * keys : (j + 1) * keys] = jnp.exp2(
                    (piece - top) * factor
                ).astype(jnp.bfloat16)

    def mix(u):
        block, m = units[u]
        span = (block + 1) * keys
        acc = jnp.dot(weights[u % 2, :, :span], vs[:span, :], preferred_element_type=jnp.float32)
        maps[m] = acc[:, :value] / acc[:, value:]
        if m == 1:
            heads_at = lax.broadcasted_iota(jnp.int32, lam.shape, 1)
            factor2 = jnp.sum(jnp.where(heads_at == z, lam[...], 0.0), axis=1, keepdims=True)
            diff = maps[0] - factor2 * maps[1]
            inverse = lax.rsqrt(jnp.mean(diff * diff, axis=1, keepdims=True) + norm_eps)
            heads[block * rows : (block + 1) * rows, :] = (diff * inverse * gain[...]).astype(
                jnp.bfloat16
            )

    score(0)
    for u in range(len(units)):
        if u + 1 < len(units):
            score(u + 1)
        if u > 0:
            mix(u - 1)
        weigh(u)
    mix(len(units) - 1)
    for s in range(count):
        outs[s][...] = heads[pl.ds(pl.multiple_of((z ^ s) * rows, rows), rows), :]


def project_kernel(*refs, count, direct):
    heads, weight, (*outs, rows_ref) = refs[:count], refs[count], refs[count + 1 :]
    z, _, ti = place()
    value = heads[0].shape[1]
    for s in range(count):
        rows_ref[:, pl.ds(pl.multiple_of((z ^ s) * value, value), value)] = heads[s][...]
    rows = rows_ref[...]
    cols = outs[0].shape[1]

    def block(n):
        at = pl.ds(pl.multiple_of(n * cols, cols), cols)
        return jnp.dot(rows, weight[:, at], preferred_element_type=jnp.float32)

    spread_out(block, ti, outs, direct)


def rotate(inputs, positions):
    half_size = inputs.shape[-1] // 2
    frequency = theta_base ** (-(jnp.arange(half_size, dtype=jnp.float32) * 2.0) / inputs.shape[-1])
    angles = positions.astype(jnp.float32)[:, None] * frequency[None, :]
    cosine = jnp.cos(angles)[:, None, None, :]
    sine_part = jnp.sin(angles)[:, None, None, :]
    front_half = inputs[..., :half_size]
    back_half = inputs[..., half_size:]
    return jnp.concatenate(
        [front_half * cosine - back_half * sine_part, back_half * cosine + front_half * sine_part],
        axis=-1,
    )


def gathered_attention(query_pairs, key_pairs, value_rows, head_lambda, head_gain):
    local_rows = query_pairs.shape[0]
    local_heads = head_lambda.shape[0]
    head_size = query_pairs.shape[1] // (2 * local_heads)
    value_size = value_rows.shape[1] // local_heads
    positions = lax.axis_index("ep") * local_rows + jnp.arange(local_rows, dtype=jnp.int32)
    rot_queries = rotate(
        query_pairs.astype(jnp.float32).reshape(local_rows, local_heads, 2, head_size), positions
    ).astype(jnp.bfloat16)
    rot_keys = rotate(
        key_pairs.astype(jnp.float32).reshape(local_rows, local_heads, 2, head_size), positions
    ).astype(jnp.bfloat16)
    rot_keys = rot_keys.reshape(local_rows, local_heads * 2 * head_size)
    zero_init = (
        jnp.full((local_heads, 2, local_rows), masked_low, jnp.float32),
        jnp.zeros((local_heads, 2, local_rows), jnp.float32),
        jnp.zeros((local_heads, 2, local_rows, value_size), jnp.float32),
    )
    piece_keys = lax.all_gather(rot_keys, "ep", axis=0, tiled=True)
    piece_values = lax.all_gather(value_rows, "ep", axis=0, tiled=True)
    block_count = piece_keys.shape[0] // KEY_BLOCK
    group_size = 4 if block_count % 4 == 0 else 1
    group_count = block_count // group_size
    grouped_keys = piece_keys.reshape(group_count, group_size, KEY_BLOCK, local_heads, 2, head_size)
    grouped_values = piece_values.reshape(
        group_count, group_size, KEY_BLOCK, local_heads, value_size
    )

    def one_group(current, inputs):
        block_keys, block_values, group_index = inputs
        key_positions = group_index * group_size * KEY_BLOCK + jnp.arange(
            group_size * KEY_BLOCK, dtype=jnp.int32
        ).reshape(group_size, KEY_BLOCK)
        scores = jnp.einsum(
            "qhmd,gkhmd->hmqgk", rot_queries, block_keys, preferred_element_type=jnp.float32
        ) * head_size ** (-0.5)
        allowed = key_positions[None, :, :] <= positions[:, None, None]
        scores = jnp.where(allowed, scores, masked_low)
        block_max = jnp.max(scores, axis=-1)
        weights = jnp.where(allowed, jnp.exp(scores - block_max[..., None]), 0.0)
        block_sum = jnp.sum(weights, axis=-1)
        block_out = jnp.einsum(
            "hmqgk,gkhc->hmqgc",
            weights.astype(jnp.bfloat16),
            block_values,
            preferred_element_type=jnp.float32,
        )
        run_max, run_sum, run_out = current
        new_max = jnp.maximum(run_max, jnp.max(block_max, axis=-1))
        old_scale = jnp.exp(run_max - new_max)
        new_scale = jnp.exp(block_max - new_max[..., None])
        run_sum = run_sum * old_scale + jnp.sum(new_scale * block_sum, axis=-1)
        run_out = run_out * old_scale[..., None] + jnp.sum(
            new_scale[..., None] * block_out, axis=-2
        )
        return ((new_max, run_sum, run_out), None)

    result, _ = lax.scan(
        one_group,
        zero_init,
        (grouped_keys, grouped_values, jnp.arange(group_count, dtype=jnp.int32)),
    )
    _, run_sum, run_out = result
    map_outputs = run_out / run_sum[..., None]
    difference = map_outputs[:, 0] - head_lambda[:, None, None] * map_outputs[:, 1]
    inverse_rms = lax.rsqrt(jnp.mean(difference * difference, axis=-1, keepdims=True) + norm_eps)
    normed_heads = (difference * inverse_rms * head_gain).astype(jnp.bfloat16)
    return [normed_heads.transpose(1, 0, 2).reshape(local_rows, local_heads * value_size)]


def inner(
    query_pairs,
    key_pairs,
    value_rows,
    head_lambda,
    head_gain,
    out_weight,
    moe_input,
    ffn_gain,
    routes,
    route_weight,
    gate_weight,
    up_weight,
    down_weight,
    shared_gate,
    shared_up,
    shared_down,
):
    ep, tp = lax.axis_size("ep"), lax.axis_size("tp")
    chips = ep // 2
    ei = lax.axis_index("ep")

    def along_z(x, s):
        return lax.ppermute(x, "ep", [(i, 2 * ((i // 2) ^ s) + i % 2) for i in range(ep)])

    def swap(x):
        return lax.ppermute(x, "ep", [(i, i ^ 1) for i in range(ep)])

    def along_tp(x, s):
        return lax.ppermute(x, "tp", [(i, i ^ s) for i in range(tp)])

    def exchange(parts, move):
        return [parts[0]] + [move(parts[s], s) for s in range(1, len(parts))]

    direct = tp != 4

    def gather_tp(own, other):
        if direct:
            return [
                piece
                for half in (own, other)
                for piece in [half] + [along_tp(half, s) for s in range(1, tp)]
            ]
        own_1, other_2 = along_tp(own, 1), along_tp(other, 2)
        own_2, other_1 = along_tp(own, 2), along_tp(other, 1)
        own_3, other_3 = along_tp(own_1, 2), along_tp(other_2, 1)
        return [own, own_1, own_2, own_3, other, other_1, other_2, other_3]

    def reduce_tp(parts):
        up = lambda x: x.astype(jnp.float32)
        if direct:
            total = sum(up(p) for p in exchange(parts, along_tp))
            half = total.shape[0] // 2
            return total[:half], total[half:]
        send_x, keep_x, send_y, keep_y = parts
        half = send_x.shape[0] // 2
        got_x, got_y = along_tp(send_x, 1), along_tp(send_y, 2)
        mid_x = (up(keep_x[half:]) + up(got_x[half:])).astype(jnp.bfloat16)
        mid_y = (up(keep_y[half:]) + up(got_y[half:])).astype(jnp.bfloat16)
        mid_x, mid_y = along_tp(mid_x, 2), along_tp(mid_y, 1)
        return (
            up(keep_x[:half]) + up(got_x[:half]) + up(mid_x),
            up(keep_y[:half]) + up(got_y[:half]) + up(mid_y),
        )

    tokens, width = moe_input.shape
    cap = tokens * TOP_K * 5 // (4 * ep)
    slice_width = width // tp
    xn, slots, *parts = pl.pallas_call(
        lambda *refs: dispatch_kernel(*refs, cap=cap, experts=ep),
        out_shape=[sds((tokens, width)), sds((TOP_K, tokens), jnp.int32)]
        + [sds((2 * cap, slice_width))] * chips,
        in_specs=[FAR] * 3,
        out_specs=[VM] * (2 + chips),
        scratch_shapes=[
            pltpu.VMEM(moe_input.shape, jnp.bfloat16),
            pltpu.VMEM((1, width), jnp.float32),
            pltpu.VMEM((TOP_K, tokens), jnp.int32),
            DMA((3,)),
        ],
        cost_estimate=cost(4e8),
        name="dispatch",
        compiler_params=limit(8),
    )(far(moe_input), far(ffn_gain.reshape(1, -1)), far(routes.T))
    arrived = exchange(parts, along_z)

    rows = query_pairs.shape[0]
    heads = head_lambda.shape[0]
    size = query_pairs.shape[1] // (2 * heads)
    value = value_rows.shape[1] // heads
    spread = heads == chips and value == 2 * size and value % 128 == 0
    if spread:
        positions = (ei * rows + jnp.arange(rows, dtype=jnp.int32)).astype(jnp.float32)
        index = jnp.arange(2 * size, dtype=jnp.int32)
        frequency = theta_base ** (-((index % (size // 2)).astype(jnp.float32) * 2.0) / size)
        angles = positions[:, None] * frequency[None, :]
        sign = jnp.where(index % size < size // 2, -1.0, 1.0).astype(jnp.float32)
        cosine = jnp.cos(angles)
        sine = jnp.sin(angles) * sign
        packs = pl.pallas_call(
            lambda *refs: rope_kernel(*refs, size=size),
            out_shape=[sds((3 * rows, value))] * chips,
            in_specs=[FAR] * 3 + [VM] * 2,
            out_specs=[VM] * chips,
            scratch_shapes=[pltpu.VMEM(query_pairs.shape, jnp.bfloat16)] * 3 + [DMA((3,))],
            cost_estimate=cost(4e8),
            name="rope",
        compiler_params=limit(8),
        )(far(query_pairs), far(key_pairs), far(value_rows), cosine, sine)
        packs = exchange(packs, along_z)
        others = [swap(packs[0])]
        others += [swap(p) for p in packs[1:]]

    shared = run_expert([xn], 1, shared_gate, shared_up, shared_down, tp, True)
    shared = exchange(shared, along_tp)

    own, other = pl.pallas_call(
        lambda *refs: pack_kernel(*refs, count=chips, cap=cap),
        out_shape=[sds((chips * cap, slice_width))] * 2,
        in_specs=[VM] * chips,
        out_specs=[VM] * 2,
        cost_estimate=cost(1e8),
        compiler_params=limit(8),
        name="pack",
    )(*arrived)
    other = swap(other)
    slices = gather_tp(own, other)
    terms = run_expert(slices, 2, gate_weight[0], up_weight[0], down_weight[0], tp, direct)
    summed = [x.astype(jnp.bfloat16) for x in reduce_tp(terms)]

    if spread:
        heads_out = pl.pallas_call(
            lambda *refs: attend_kernel(*refs, count=chips, rows=rows, size=size),
            out_shape=[sds((rows, value))] * chips,
            in_specs=[FAR, FAR] + [ANY] * (2 * chips),
            out_specs=[VM] * chips,
            scratch_shapes=[
                pltpu.VMEM((chips * rows, value), jnp.bfloat16),
                pltpu.VMEM((ep * rows, value), jnp.bfloat16),
                pltpu.VMEM((ep * rows, 2 * value), jnp.bfloat16),
                pltpu.VMEM((2, rows, ep * rows), jnp.float32),
                pltpu.VMEM((2, rows, ep * rows), jnp.bfloat16),
                pltpu.VMEM((chips * rows, value), jnp.bfloat16),
                pltpu.VMEM((1, heads), jnp.float32),
                pltpu.VMEM((1, value), jnp.float32),
                DMA((5 * chips + 2,)),
            ],
            cost_estimate=cost(4e9),
            name="attend",
        compiler_params=limit(32),
        )(head_lambda.reshape(1, -1), head_gain.reshape(1, -1), *packs, *others)
        normed = exchange(heads_out, along_z)
        shapes = out_shapes(rows, out_weight.shape[1] // tp, tp, direct)
        mixer = pl.pallas_call(
            lambda *refs: project_kernel(*refs, count=chips, direct=direct),
            out_shape=shapes,
            in_specs=[VM] * (chips + 1),
            out_specs=[VM] * len(shapes),
            scratch_shapes=[pltpu.VMEM((rows, chips * value), jnp.bfloat16)],
            cost_estimate=cost(1e9),
            name="project",
            compiler_params=limit(12),
        )(*normed, out_weight)
        attn_out = jnp.concatenate(reduce_tp(mixer), axis=0).astype(jnp.bfloat16)
    else:
        head_rows = gathered_attention(query_pairs, key_pairs, value_rows, head_lambda, head_gain)[0]
        mixer = jnp.dot(head_rows, out_weight, preferred_element_type=jnp.float32)
        attn_out = lax.psum_scatter(
            mixer.astype(jnp.bfloat16), "tp", scatter_dimension=1, tiled=True
        )

    back = swap(summed[1])
    groups = [
        jnp.concatenate([x[s * cap : (s + 1) * cap] for x in (summed[0], back)], axis=0)
        for s in range(chips)
    ]
    groups = exchange(groups, along_z)
    moe_out = pl.pallas_call(
        lambda *refs: combine_kernel(*refs, count=chips),
        out_shape=sds((tokens, slice_width)),
        in_specs=[VM] * (2 + chips + tp),
        out_specs=VM,
        cost_estimate=cost(4e8),
        name="combine",
        compiler_params=limit(10),
    )(slots, route_weight.T, *groups, *shared)
    return (attn_out, moe_out)


def solution(mesh):
    return jax.shard_map(
        inner,
        mesh=mesh,
        in_specs=(
            P("ep", "tp"),
            P("ep", "tp"),
            P("ep", "tp"),
            P("tp"),
            P(),
            P("tp", None),
            P("ep", None),
            P(),
            P("ep", None),
            P("ep", None),
            P("ep", None, "tp"),
            P("ep", None, "tp"),
            P("ep", "tp", None),
            P(None, "tp"),
            P(None, "tp"),
            P("tp", None),
        ),
        out_specs=(P("ep", "tp"), P("ep", "tp")),
        check_vma=False,
    )
```

```python
import math

import jax
import jax.numpy as jnp
from jax import lax
from jax.experimental import pallas as pl
from jax.experimental.pallas import tpu as pltpu
from jax.sharding import PartitionSpec as P


TOP_K = 2
KEY_BLOCK = 128

theta_base = 500000.0
norm_eps = 1e-06
masked_low = -1e30
LOG2E = 1.4426950408889634

VM = pl.BlockSpec(memory_space=pltpu.VMEM)
SM = pl.BlockSpec(memory_space=pltpu.SMEM)
ANY = pl.BlockSpec(memory_space=pl.ANY)
FAR = pl.BlockSpec(memory_space=pltpu.HBM)
DMA = pltpu.SemaphoreType.DMA


def sds(shape, dtype=jnp.bfloat16):
    return jax.ShapeDtypeStruct(shape, dtype)


def limit(mib):
    return pltpu.CompilerParams(vmem_limit_bytes=mib * 1024 * 1024)


def far(x):
    return pltpu.with_memory_space_constraint(x, pltpu.HBM)


def begin(pairs, sems):
    copies = [pltpu.make_async_copy(a, b, sems.at[n]) for n, (a, b) in enumerate(pairs)]
    for copy in copies:
        copy.start()
    return copies


def cost(flops):
    return pl.CostEstimate(flops=int(flops), bytes_accessed=0, transcendentals=0)


def place():
    ei = lax.axis_index("ep")
    return ei // 2, ei % 2, lax.axis_index("tp")


def column(row):
    n = row.shape[1]
    at = lax.broadcasted_iota(jnp.int32, (n, n), 0)
    diagonal = at == lax.broadcasted_iota(jnp.int32, (n, n), 1)
    return jnp.sum(jnp.where(diagonal, row, jnp.zeros_like(row)), axis=1, keepdims=True)


def dispatch_kernel(rows_far, gain_far, routes_far, xn_out, slots_out, *refs, cap, experts):
    *parts, rows, gain, routes, sems = refs
    z, core, ti = place()
    tokens = rows.shape[0]
    for copy in begin(((rows_far, rows), (gain_far, gain), (routes_far, routes)), sems):
        copy.wait()
    values = rows[...].astype(jnp.float32)
    inverse = lax.rsqrt(jnp.mean(values * values, axis=-1, keepdims=True) + norm_eps)
    xn_out[...] = (values * inverse * gain[...]).astype(jnp.bfloat16)
    group = 2 * cap
    t_row = lax.broadcasted_iota(jnp.int32, (tokens, tokens), 0)
    t_col = lax.broadcasted_iota(jnp.int32, (tokens, tokens), 1)
    e_row = lax.broadcasted_iota(jnp.int32, (experts, tokens), 0)
    before = (t_row < t_col).astype(jnp.float32).astype(jnp.bfloat16)
    hits = [(e_row == routes[k : k + 1, :]).astype(jnp.float32) for k in range(TOP_K)]
    count = jnp.dot(sum(hits).astype(jnp.bfloat16), before, preferred_element_type=jnp.float32)
    slots = []
    for k in range(TOP_K):
        expert = routes[k : k + 1, :]
        rank = jnp.sum(count * hits[k], axis=0, keepdims=True).astype(jnp.int32)
        slots.append(((expert // 2) ^ z) * group + ((expert % 2) ^ core) * cap + rank)
        slots_out[k : k + 1, :] = slots[k]
    width = parts[0].shape[1]
    mine = xn_out[:, pl.ds(pl.multiple_of(ti * width, width), width)]
    for s, part in enumerate(parts):
        slot_row = lax.broadcasted_iota(jnp.int32, (group, tokens), 0) + s * group
        pick = slot_row == slots[0]
        for k in range(1, TOP_K):
            pick = pick | (slot_row == slots[k])
        pick = pick.astype(jnp.float32).astype(jnp.bfloat16)
        part[...] = jnp.dot(pick, mine, preferred_element_type=jnp.float32).astype(jnp.bfloat16)


def pack_kernel(*refs, count, cap):
    parts, own, other = refs[:count], refs[count], refs[count + 1]
    for s in range(count):
        own[s * cap : (s + 1) * cap, :] = parts[s][:cap, :]
        other[s * cap : (s + 1) * cap, :] = parts[s][cap:, :]


def spread_out(block, ti, outs, direct):
    def put(ref, at, pieces):
        for piece in pieces:
            ref[at : at + piece.shape[0], :] = piece.astype(jnp.bfloat16)
            at += piece.shape[0]

    if direct:
        for s, out in enumerate(outs):
            upper, lower = block(ti ^ s)
            put(out, 0, upper + lower)
        return
    send_x, keep_x, send_y, keep_y = outs
    half = send_x.shape[0] // 2
    places = (
        (0, (keep_x, 0), (keep_y, 0)),
        (1, (send_x, 0), (keep_y, half)),
        (2, (keep_x, half), (send_y, 0)),
        (3, (send_x, half), (send_y, half)),
    )
    for s, above, below in places:
        upper, lower = block(ti ^ s)
        put(*above, upper)
        put(*below, lower)


def halves_of(values):
    half = values.shape[0] // 2
    return values[:half], values[half:]


def expert_kernel(*refs, pieces, halves, direct, staged, extra):
    ti = place()[2]
    if extra:
        added, refs = refs[0], refs[1:]
    xs, (gate_w, up_w, down_w) = refs[: pieces * halves], refs[pieces * halves :][:3]
    rest = refs[pieces * halves + 3 :]
    chunks = pieces
    if staged:
        *ys, rows_ref, gates, ups, downs, sems = rest
        chunks = gates.shape[0]
        width = gates.shape[1]
        pairs = []
        for s in range(chunks):
            at = pl.ds(pl.multiple_of((ti ^ s) * width, width), width)
            pairs += [(gate_w.at[at, :], gates.at[s]), (up_w.at[at, :], ups.at[s])]
        copies = begin(pairs + [(down_w, downs)], sems)
    else:
        *ys, rows_ref = rest
        width = gate_w.shape[0] // chunks
        downs = down_w
    gate = up = None
    for s in range(chunks):
        part = xs[0].shape[0]
        at = pl.ds(pl.multiple_of((ti ^ s) * width, width), width)
        if pieces == 1:
            x = xs[0][:, at]
        else:
            for h in range(halves):
                rows_ref[s % 2, h * part : (h + 1) * part, :] = xs[h * pieces + s][...]
            x = rows_ref[s % 2]
        if staged:
            copies[2 * s].wait()
            copies[2 * s + 1].wait()
            wg, wu = gates[s], ups[s]
        else:
            wg, wu = gate_w[at, :], up_w[at, :]
        g = jnp.dot(x, wg, preferred_element_type=jnp.float32)
        u = jnp.dot(x, wu, preferred_element_type=jnp.float32)
        gate = g if gate is None else gate + g
        up = u if up is None else up + u
    hidden = (gate / (1.0 + jnp.exp(-gate)) * up).astype(jnp.bfloat16)
    if staged:
        copies[-1].wait()
    if staged:
        ys[0][...] = jnp.dot(hidden, downs[...], preferred_element_type=jnp.float32).astype(
            jnp.bfloat16
        )
        return
    cols = ys[0].shape[1]

    def block(n):
        at = pl.ds(pl.multiple_of(n * cols, cols), cols)
        above, below = halves_of(jnp.dot(hidden, downs[:, at], preferred_element_type=jnp.float32))
        if not extra:
            return [above], [below]
        more_above, more_below = halves_of(added[:, at])
        return [above, more_above], [below, more_below]

    spread_out(block, ti, ys, direct)


def out_shapes(rows, cols, tp, direct):
    return [sds((rows, cols))] * (tp if direct else 4)


def run_expert(xs, halves, gate_w, up_w, down_w, tp, direct, extra=()):
    rows = xs[0].shape[0] * halves
    width, hidden = gate_w.shape
    pieces = len(xs) // halves
    staged = pieces == 1
    if staged:
        shapes = [sds((rows, down_w.shape[1]))]
    else:
        total = rows + sum(x.shape[0] for x in extra)
        shapes = out_shapes(total, down_w.shape[1] // tp, tp, direct)
    scratch = [pltpu.VMEM((2, rows, width // tp), jnp.bfloat16)]
    if staged:
        part = pltpu.VMEM((tp, width // tp, hidden), jnp.bfloat16)
        scratch += [part, part, pltpu.VMEM(down_w.shape, jnp.bfloat16), DMA((2 * tp + 1,))]
        gate_w, up_w, down_w = far(gate_w), far(up_w), far(down_w)
    return pl.pallas_call(
        lambda *refs: expert_kernel(
            *refs,
            pieces=pieces,
            halves=halves,
            direct=direct,
            staged=staged,
            extra=len(extra) > 0,
        ),
        out_shape=shapes,
        in_specs=[VM] * (len(extra) + len(xs)) + [FAR if staged else VM] * 3,
        out_specs=[VM] * len(shapes),
        scratch_shapes=scratch,
        cost_estimate=cost(6 * rows * width * hidden),
        compiler_params=limit(24),
    )(*extra, *xs, gate_w, up_w, down_w)


def combine_kernel(slots, weights, *refs, count):
    back, shared, out = refs[:count], refs[count:-1], refs[-1]
    tokens = slots.shape[1]
    own = [column(slots[k : k + 1, :]) for k in range(TOP_K)]
    scale = [column(weights[k : k + 1, :]) for k in range(TOP_K)]
    group = back[0].shape[0]
    total = jnp.concatenate([part[...] for part in shared], axis=0)
    picked = [None] * TOP_K
    for s in range(count):
        slot_col = lax.broadcasted_iota(jnp.int32, (tokens, group), 1) + s * group
        rows = back[s][...]
        for k in range(TOP_K):
            pick = (slot_col == own[k]).astype(jnp.float32).astype(jnp.bfloat16)
            term = jnp.dot(pick, rows, preferred_element_type=jnp.float32)
            picked[k] = term if picked[k] is None else picked[k] + term
    routed = scale[0] * picked[0]
    for k in range(1, TOP_K):
        routed = routed + scale[k] * picked[k]
    out[...] = (routed + total).astype(jnp.bfloat16)


def rope_kernel(q_far, k_far, v_far, cosine, sine, *refs, size):
    *outs, q, k, v, sems = refs
    copies = begin(((q_far, q), (k_far, k), (v_far, v)), sems)
    z = place()[0]
    rows = q.shape[0]
    both = cosine.shape[1]
    half = size // 2
    lane = lax.broadcasted_iota(jnp.int32, (rows, both), 1)
    front = (lane % size) < half
    c, s_ = cosine[...], sine[...]
    for copy in copies:
        copy.wait()
    for s, out in enumerate(outs):
        at = pl.ds(pl.multiple_of((z ^ s) * both, both), both)
        for n, ref in enumerate((q, k)):
            x = ref[:, at].astype(jnp.float32)
            turned = jnp.where(front, pltpu.roll(x, both - half, 1), pltpu.roll(x, half, 1))
            out[n * rows : (n + 1) * rows, :] = (x * c + turned * s_).astype(jnp.bfloat16)
        out[2 * rows : 3 * rows, :] = v[:, at]


def attend_kernel(lam_far, gain_far, *refs, count, rows, size):
    own, other, outs = refs[:count], refs[count : 2 * count], refs[2 * count : 3 * count]
    qs, ks, vs, scores, weights, heads, lam, gain, sems = refs[3 * count :]
    z, core, _ = place()
    both = 2 * size
    value = vs.shape[1] // 2
    keys = 2 * rows
    pairs = [(lam_far, lam), (gain_far, gain)]
    for s in range(count):
        at = pl.multiple_of((z ^ s) * rows, rows)
        mine = pl.multiple_of((2 * (z ^ s) + core) * rows, rows)
        theirs = pl.multiple_of((2 * (z ^ s) + 1 - core) * rows, rows)
        pairs.append((own[s].at[pl.ds(0, rows), :], qs.at[pl.ds(at, rows), :]))
        for ref, to in ((own[s], mine), (other[s], theirs)):
            k_rows, v_rows, to = pl.ds(rows, rows), pl.ds(2 * rows, rows), pl.ds(to, rows)
            pairs.append((ref.at[k_rows, :], ks.at[to, :]))
            pairs.append((ref.at[v_rows, :], vs.at[to, pl.ds(0, value)]))
    copies = begin(pairs, sems)
    vs[:, value:] = jnp.ones((vs.shape[0], value), jnp.bfloat16)
    for copy in copies:
        copy.wait()
    factor = LOG2E * size ** (-0.5)
    lane = lax.broadcasted_iota(jnp.int32, (rows, both), 1)
    tile = math.gcd(rows, 64)
    ahead = lax.broadcasted_iota(jnp.int32, (tile, keys), 1) - lax.broadcasted_iota(
        jnp.int32, (tile, keys), 0
    )
    contract = (((1,), (1,)), ((), ()))
    units = [(block, m) for block in reversed(range(count)) for m in range(2)]
    maps = {}

    def score(u):
        block, m = units[u]
        q = qs[block * rows : (block + 1) * rows, :]
        q = jnp.where((lane < size) == (m == 0), q, jnp.zeros_like(q))
        for j in range(block + 1):
            at = slice(j * keys, (j + 1) * keys)
            scores[u % 2, :, at] = lax.dot_general(
                q, ks[at, :], contract, preferred_element_type=jnp.float32
            )

    def weigh(u):
        block, _ = units[u]
        for r in range(0, rows, tile):
            pieces = []
            for j in range(block + 1):
                piece = scores[u % 2, r : r + tile, j * keys : (j + 1) * keys]
                if j == block:
                    piece = jnp.where(ahead <= core * rows + r, piece, masked_low)
                pieces.append(piece)
            top = None
            for piece in pieces:
                one = jnp.max(piece, axis=1, keepdims=True)
                top = one if top is None else jnp.maximum(top, one)
            for j, piece in enumerate(pieces):
                weights[u % 2, r : r + tile, j * keys : (j + 1) * keys] = jnp.exp2(
                    (piece - top) * factor
                ).astype(jnp.bfloat16)

    def mix(u):
        block, m = units[u]
        span = (block + 1) * keys
        acc = jnp.dot(weights[u % 2, :, :span], vs[:span, :], preferred_element_type=jnp.float32)
        maps[m] = acc[:, :value] / acc[:, value:]
        if m == 1:
            heads_at = lax.broadcasted_iota(jnp.int32, lam.shape, 1)
            factor2 = jnp.sum(jnp.where(heads_at == z, lam[...], 0.0), axis=1, keepdims=True)
            diff = maps[0] - factor2 * maps[1]
            inverse = lax.rsqrt(jnp.mean(diff * diff, axis=1, keepdims=True) + norm_eps)
            heads[block * rows : (block + 1) * rows, :] = (diff * inverse * gain[...]).astype(
                jnp.bfloat16
            )

    score(0)
    for u in range(len(units)):
        if u + 1 < len(units):
            score(u + 1)
        if u > 0:
            mix(u - 1)
        weigh(u)
    mix(len(units) - 1)
    for s in range(count):
        outs[s][...] = heads[pl.ds(pl.multiple_of((z ^ s) * rows, rows), rows), :]


def project_kernel(*refs, count, direct):
    heads, weight, (*outs, rows_ref) = refs[:count], refs[count], refs[count + 1 :]
    z, _, ti = place()
    value = heads[0].shape[1]
    for s in range(count):
        rows_ref[:, pl.ds(pl.multiple_of((z ^ s) * value, value), value)] = heads[s][...]
    rows = rows_ref[...]
    cols = outs[0].shape[1]

    def block(n):
        at = pl.ds(pl.multiple_of(n * cols, cols), cols)
        above, below = halves_of(jnp.dot(rows, weight[:, at], preferred_element_type=jnp.float32))
        return [above], [below]

    spread_out(block, ti, outs, direct)


def rotate(inputs, positions):
    half_size = inputs.shape[-1] // 2
    frequency = theta_base ** (-(jnp.arange(half_size, dtype=jnp.float32) * 2.0) / inputs.shape[-1])
    angles = positions.astype(jnp.float32)[:, None] * frequency[None, :]
    cosine = jnp.cos(angles)[:, None, None, :]
    sine_part = jnp.sin(angles)[:, None, None, :]
    front_half = inputs[..., :half_size]
    back_half = inputs[..., half_size:]
    return jnp.concatenate(
        [front_half * cosine - back_half * sine_part, back_half * cosine + front_half * sine_part],
        axis=-1,
    )


def gathered_attention(query_pairs, key_pairs, value_rows, head_lambda, head_gain):
    local_rows = query_pairs.shape[0]
    local_heads = head_lambda.shape[0]
    head_size = query_pairs.shape[1] // (2 * local_heads)
    value_size = value_rows.shape[1] // local_heads
    positions = lax.axis_index("ep") * local_rows + jnp.arange(local_rows, dtype=jnp.int32)
    rot_queries = rotate(
        query_pairs.astype(jnp.float32).reshape(local_rows, local_heads, 2, head_size), positions
    ).astype(jnp.bfloat16)
    rot_keys = rotate(
        key_pairs.astype(jnp.float32).reshape(local_rows, local_heads, 2, head_size), positions
    ).astype(jnp.bfloat16)
    rot_keys = rot_keys.reshape(local_rows, local_heads * 2 * head_size)
    zero_init = (
        jnp.full((local_heads, 2, local_rows), masked_low, jnp.float32),
        jnp.zeros((local_heads, 2, local_rows), jnp.float32),
        jnp.zeros((local_heads, 2, local_rows, value_size), jnp.float32),
    )
    piece_keys = lax.all_gather(rot_keys, "ep", axis=0, tiled=True)
    piece_values = lax.all_gather(value_rows, "ep", axis=0, tiled=True)
    block_count = piece_keys.shape[0] // KEY_BLOCK
    group_size = 4 if block_count % 4 == 0 else 1
    group_count = block_count // group_size
    grouped_keys = piece_keys.reshape(group_count, group_size, KEY_BLOCK, local_heads, 2, head_size)
    grouped_values = piece_values.reshape(
        group_count, group_size, KEY_BLOCK, local_heads, value_size
    )

    def one_group(current, inputs):
        block_keys, block_values, group_index = inputs
        key_positions = group_index * group_size * KEY_BLOCK + jnp.arange(
            group_size * KEY_BLOCK, dtype=jnp.int32
        ).reshape(group_size, KEY_BLOCK)
        scores = jnp.einsum(
            "qhmd,gkhmd->hmqgk", rot_queries, block_keys, preferred_element_type=jnp.float32
        ) * head_size ** (-0.5)
        allowed = key_positions[None, :, :] <= positions[:, None, None]
        scores = jnp.where(allowed, scores, masked_low)
        block_max = jnp.max(scores, axis=-1)
        weights = jnp.where(allowed, jnp.exp(scores - block_max[..., None]), 0.0)
        block_sum = jnp.sum(weights, axis=-1)
        block_out = jnp.einsum(
            "hmqgk,gkhc->hmqgc",
            weights.astype(jnp.bfloat16),
            block_values,
            preferred_element_type=jnp.float32,
        )
        run_max, run_sum, run_out = current
        new_max = jnp.maximum(run_max, jnp.max(block_max, axis=-1))
        old_scale = jnp.exp(run_max - new_max)
        new_scale = jnp.exp(block_max - new_max[..., None])
        run_sum = run_sum * old_scale + jnp.sum(new_scale * block_sum, axis=-1)
        run_out = run_out * old_scale[..., None] + jnp.sum(
            new_scale[..., None] * block_out, axis=-2
        )
        return ((new_max, run_sum, run_out), None)

    result, _ = lax.scan(
        one_group,
        zero_init,
        (grouped_keys, grouped_values, jnp.arange(group_count, dtype=jnp.int32)),
    )
    _, run_sum, run_out = result
    map_outputs = run_out / run_sum[..., None]
    difference = map_outputs[:, 0] - head_lambda[:, None, None] * map_outputs[:, 1]
    inverse_rms = lax.rsqrt(jnp.mean(difference * difference, axis=-1, keepdims=True) + norm_eps)
    normed_heads = (difference * inverse_rms * head_gain).astype(jnp.bfloat16)
    return [normed_heads.transpose(1, 0, 2).reshape(local_rows, local_heads * value_size)]


def inner(
    query_pairs,
    key_pairs,
    value_rows,
    head_lambda,
    head_gain,
    out_weight,
    moe_input,
    ffn_gain,
    routes,
    route_weight,
    gate_weight,
    up_weight,
    down_weight,
    shared_gate,
    shared_up,
    shared_down,
):
    ep, tp = lax.axis_size("ep"), lax.axis_size("tp")
    chips = ep // 2
    ei = lax.axis_index("ep")

    def along_z(x, s):
        return lax.ppermute(x, "ep", [(i, 2 * ((i // 2) ^ s) + i % 2) for i in range(ep)])

    def swap(x):
        return lax.ppermute(x, "ep", [(i, i ^ 1) for i in range(ep)])

    def along_tp(x, s):
        return lax.ppermute(x, "tp", [(i, i ^ s) for i in range(tp)])

    def exchange(parts, move, near_first=False):
        moved = {}
        turns = range(1, len(parts))
        for s in turns if near_first else reversed(turns):
            moved[s] = move(parts[s], s)
        return [parts[0]] + [moved[s] for s in range(1, len(parts))]

    direct = tp != 4

    def gather_tp(own, other):
        if direct:
            return [
                piece
                for half in (own, other)
                for piece in [half] + [along_tp(half, s) for s in range(1, tp)]
            ]
        own_1, other_2 = along_tp(own, 1), along_tp(other, 2)
        own_2, other_1 = along_tp(own, 2), along_tp(other, 1)
        own_3, other_3 = along_tp(own_1, 2), along_tp(other_2, 1)
        return [own, own_1, own_2, own_3, other, other_1, other_2, other_3]

    def reduce_tp(parts):
        up = lambda x: x.astype(jnp.float32)
        if direct:
            total = sum(up(p) for p in exchange(parts, along_tp))
            half = total.shape[0] // 2
            return total[:half], total[half:]
        send_x, keep_x, send_y, keep_y = parts
        half = send_x.shape[0] // 2
        got_x, got_y = along_tp(send_x, 1), along_tp(send_y, 2)
        mid_x = (up(keep_x[half:]) + up(got_x[half:])).astype(jnp.bfloat16)
        mid_y = (up(keep_y[half:]) + up(got_y[half:])).astype(jnp.bfloat16)
        mid_x, mid_y = along_tp(mid_x, 2), along_tp(mid_y, 1)
        return (
            up(keep_x[:half]) + up(got_x[:half]) + up(mid_x),
            up(keep_y[:half]) + up(got_y[:half]) + up(mid_y),
        )

    tokens, width = moe_input.shape
    cap = tokens * TOP_K * 5 // (4 * ep)
    slice_width = width // tp
    xn, slots, *parts = pl.pallas_call(
        lambda *refs: dispatch_kernel(*refs, cap=cap, experts=ep),
        out_shape=[sds((tokens, width)), sds((TOP_K, tokens), jnp.int32)]
        + [sds((2 * cap, slice_width))] * chips,
        in_specs=[FAR] * 3,
        out_specs=[VM] * (2 + chips),
        scratch_shapes=[
            pltpu.VMEM(moe_input.shape, jnp.bfloat16),
            pltpu.VMEM((1, width), jnp.float32),
            pltpu.VMEM((TOP_K, tokens), jnp.int32),
            DMA((3,)),
        ],
        cost_estimate=cost(4e8),
        name="dispatch",
        compiler_params=limit(8),
    )(far(moe_input), far(ffn_gain.reshape(1, -1)), far(routes.T))
    arrived = exchange(parts, along_z)

    rows = query_pairs.shape[0]
    heads = head_lambda.shape[0]
    size = query_pairs.shape[1] // (2 * heads)
    value = value_rows.shape[1] // heads
    spread = heads == chips and value == 2 * size and value % 128 == 0
    if spread:
        positions = (ei * rows + jnp.arange(rows, dtype=jnp.int32)).astype(jnp.float32)
        index = jnp.arange(2 * size, dtype=jnp.int32)
        frequency = theta_base ** (-((index % (size // 2)).astype(jnp.float32) * 2.0) / size)
        angles = positions[:, None] * frequency[None, :]
        sign = jnp.where(index % size < size // 2, -1.0, 1.0).astype(jnp.float32)
        cosine = jnp.cos(angles)
        sine = jnp.sin(angles) * sign
        packs = pl.pallas_call(
            lambda *refs: rope_kernel(*refs, size=size),
            out_shape=[sds((3 * rows, value))] * chips,
            in_specs=[FAR] * 3 + [VM] * 2,
            out_specs=[VM] * chips,
            scratch_shapes=[pltpu.VMEM(query_pairs.shape, jnp.bfloat16)] * 3 + [DMA((3,))],
            cost_estimate=cost(4e8),
            name="rope",
        compiler_params=limit(8),
        )(far(query_pairs), far(key_pairs), far(value_rows), cosine, sine)
        packs = exchange(packs, along_z, near_first=True)
        others = [swap(packs[0])]
        for s in range(1, chips):
            others.append(swap(packs[s]))

    shared = run_expert([xn], 1, shared_gate, shared_up, shared_down, tp, True)
    own, other = pl.pallas_call(
        lambda *refs: pack_kernel(*refs, count=chips, cap=cap),
        out_shape=[sds((chips * cap, slice_width))] * 2,
        in_specs=[VM] * chips,
        out_specs=[VM] * 2,
        cost_estimate=cost(1e8),
        compiler_params=limit(8),
        name="pack",
    )(*arrived)
    other = swap(other)
    slices = gather_tp(own, other)
    terms = run_expert(
        slices, 2, gate_weight[0], up_weight[0], down_weight[0], tp, direct, extra=shared
    )
    summed = reduce_tp(terms)
    routed = chips * cap
    shared = [x[routed:] for x in summed]
    summed = [x[:routed].astype(jnp.bfloat16) for x in summed]

    if spread:
        heads_out = pl.pallas_call(
            lambda *refs: attend_kernel(*refs, count=chips, rows=rows, size=size),
            out_shape=[sds((rows, value))] * chips,
            in_specs=[FAR, FAR] + [ANY] * (2 * chips),
            out_specs=[VM] * chips,
            scratch_shapes=[
                pltpu.VMEM((chips * rows, value), jnp.bfloat16),
                pltpu.VMEM((ep * rows, value), jnp.bfloat16),
                pltpu.VMEM((ep * rows, 2 * value), jnp.bfloat16),
                pltpu.VMEM((2, rows, ep * rows), jnp.float32),
                pltpu.VMEM((2, rows, ep * rows), jnp.bfloat16),
                pltpu.VMEM((chips * rows, value), jnp.bfloat16),
                pltpu.VMEM((1, heads), jnp.float32),
                pltpu.VMEM((1, value), jnp.float32),
                DMA((5 * chips + 2,)),
            ],
            cost_estimate=cost(4e9),
            name="attend",
        compiler_params=limit(32),
        )(head_lambda.reshape(1, -1), head_gain.reshape(1, -1), *packs, *others)
        normed = exchange(heads_out, along_z)
        shapes = out_shapes(rows, out_weight.shape[1] // tp, tp, direct)
        mixer = pl.pallas_call(
            lambda *refs: project_kernel(*refs, count=chips, direct=direct),
            out_shape=shapes,
            in_specs=[VM] * (chips + 1),
            out_specs=[VM] * len(shapes),
            scratch_shapes=[pltpu.VMEM((rows, chips * value), jnp.bfloat16)],
            cost_estimate=cost(1e9),
            name="project",
            compiler_params=limit(12),
        )(*normed, out_weight)
        attn_out = jnp.concatenate(reduce_tp(mixer), axis=0).astype(jnp.bfloat16)
    else:
        head_rows = gathered_attention(query_pairs, key_pairs, value_rows, head_lambda, head_gain)[0]
        mixer = jnp.dot(head_rows, out_weight, preferred_element_type=jnp.float32)
        attn_out = lax.psum_scatter(
            mixer.astype(jnp.bfloat16), "tp", scatter_dimension=1, tiled=True
        )

    back = swap(summed[1])
    groups = [
        jnp.concatenate([x[s * cap : (s + 1) * cap] for x in (summed[0], back)], axis=0)
        for s in range(chips)
    ]
    groups = exchange(groups, along_z)
    moe_out = pl.pallas_call(
        lambda *refs: combine_kernel(*refs, count=chips),
        out_shape=sds((tokens, slice_width)),
        in_specs=[VM] * (2 + chips + len(shared)),
        out_specs=VM,
        cost_estimate=cost(4e8),
        name="combine",
        compiler_params=limit(10),
    )(slots, route_weight.T, *groups, *shared)
    return (attn_out, moe_out)


def solution(mesh):
    return jax.shard_map(
        inner,
        mesh=mesh,
        in_specs=(
            P("ep", "tp"),
            P("ep", "tp"),
            P("ep", "tp"),
            P("tp"),
            P(),
            P("tp", None),
            P("ep", None),
            P(),
            P("ep", None),
            P("ep", None),
            P("ep", None, "tp"),
            P("ep", None, "tp"),
            P("ep", "tp", None),
            P(None, "tp"),
            P(None, "tp"),
            P("tp", None),
        ),
        out_specs=(P("ep", "tp"), P("ep", "tp")),
        check_vma=False,
    )
```

```python
import math

import jax
import jax.numpy as jnp
from jax import lax
from jax.experimental import pallas as pl
from jax.experimental.pallas import tpu as pltpu
from jax.sharding import PartitionSpec as P


TOP_K = 2
KEY_BLOCK = 128

theta_base = 500000.0
norm_eps = 1e-06
masked_low = -1e30
LOG2E = 1.4426950408889634

VM = pl.BlockSpec(memory_space=pltpu.VMEM)
SM = pl.BlockSpec(memory_space=pltpu.SMEM)
ANY = pl.BlockSpec(memory_space=pl.ANY)
FAR = pl.BlockSpec(memory_space=pltpu.HBM)
DMA = pltpu.SemaphoreType.DMA


def sds(shape, dtype=jnp.bfloat16):
    return jax.ShapeDtypeStruct(shape, dtype)


def limit(mib):
    return pltpu.CompilerParams(vmem_limit_bytes=mib * 1024 * 1024)


def far(x):
    return pltpu.with_memory_space_constraint(x, pltpu.HBM)


def begin(pairs, sems):
    copies = [pltpu.make_async_copy(a, b, sems.at[n]) for n, (a, b) in enumerate(pairs)]
    for copy in copies:
        copy.start()
    return copies


def cost(flops):
    return pl.CostEstimate(flops=int(flops), bytes_accessed=0, transcendentals=0)


def place():
    ei = lax.axis_index("ep")
    return ei // 2, ei % 2, lax.axis_index("tp")


def column(row):
    n = row.shape[1]
    at = lax.broadcasted_iota(jnp.int32, (n, n), 0)
    diagonal = at == lax.broadcasted_iota(jnp.int32, (n, n), 1)
    return jnp.sum(jnp.where(diagonal, row, jnp.zeros_like(row)), axis=1, keepdims=True)


def dispatch_kernel(rows_far, gain_far, routes_far, xn_out, slots_out, *refs, cap, experts):
    *parts, rows, gain, routes, sems = refs
    z, core, ti = place()
    tokens = rows.shape[0]
    for copy in begin(((rows_far, rows), (gain_far, gain), (routes_far, routes)), sems):
        copy.wait()
    values = rows[...].astype(jnp.float32)
    inverse = lax.rsqrt(jnp.mean(values * values, axis=-1, keepdims=True) + norm_eps)
    xn_out[...] = (values * inverse * gain[...]).astype(jnp.bfloat16)
    group = 2 * cap
    t_row = lax.broadcasted_iota(jnp.int32, (tokens, tokens), 0)
    t_col = lax.broadcasted_iota(jnp.int32, (tokens, tokens), 1)
    e_row = lax.broadcasted_iota(jnp.int32, (experts, tokens), 0)
    before = (t_row < t_col).astype(jnp.float32).astype(jnp.bfloat16)
    hits = [(e_row == routes[k : k + 1, :]).astype(jnp.float32) for k in range(TOP_K)]
    count = jnp.dot(sum(hits).astype(jnp.bfloat16), before, preferred_element_type=jnp.float32)
    slots = []
    for k in range(TOP_K):
        expert = routes[k : k + 1, :]
        rank = jnp.sum(count * hits[k], axis=0, keepdims=True).astype(jnp.int32)
        slots.append(((expert // 2) ^ z) * group + ((expert % 2) ^ core) * cap + rank)
        slots_out[k : k + 1, :] = slots[k]
    width = parts[0].shape[1]
    mine = xn_out[:, pl.ds(pl.multiple_of(ti * width, width), width)]
    for s, part in enumerate(parts):
        slot_row = lax.broadcasted_iota(jnp.int32, (group, tokens), 0) + s * group
        pick = slot_row == slots[0]
        for k in range(1, TOP_K):
            pick = pick | (slot_row == slots[k])
        pick = pick.astype(jnp.float32).astype(jnp.bfloat16)
        part[...] = jnp.dot(pick, mine, preferred_element_type=jnp.float32).astype(jnp.bfloat16)


def pack_kernel(*refs, count, cap):
    parts, own, other = refs[:count], refs[count], refs[count + 1]
    for s in range(count):
        own[s * cap : (s + 1) * cap, :] = parts[s][:cap, :]
        other[s * cap : (s + 1) * cap, :] = parts[s][cap:, :]


def spread_out(block, ti, outs, direct):
    def put(ref, at, pieces):
        for piece in pieces:
            ref[at : at + piece.shape[0], :] = piece.astype(jnp.bfloat16)
            at += piece.shape[0]

    if direct:
        for s, out in enumerate(outs):
            upper, lower = block(ti ^ s)
            put(out, 0, upper + lower)
        return
    send_x, keep_x, send_y, keep_y = outs
    half = send_x.shape[0] // 2
    places = (
        (0, (keep_x, 0), (keep_y, 0)),
        (1, (send_x, 0), (keep_y, half)),
        (2, (keep_x, half), (send_y, 0)),
        (3, (send_x, half), (send_y, half)),
    )
    for s, above, below in places:
        upper, lower = block(ti ^ s)
        put(*above, upper)
        put(*below, lower)


def halves_of(values):
    half = values.shape[0] // 2
    return values[:half], values[half:]


def expert_kernel(*refs, pieces, halves, direct, staged, extra):
    ti = place()[2]
    if extra:
        added, refs = refs[0], refs[1:]
    xs, (gate_w, up_w, down_w) = refs[: pieces * halves], refs[pieces * halves :][:3]
    rest = refs[pieces * halves + 3 :]
    chunks = pieces
    if staged:
        *ys, rows_ref, gates, ups, downs, sems = rest
        chunks = gates.shape[0]
        width = gates.shape[1]
        pairs = []
        for s in range(chunks):
            at = pl.ds(pl.multiple_of((ti ^ s) * width, width), width)
            pairs += [(gate_w.at[at, :], gates.at[s]), (up_w.at[at, :], ups.at[s])]
        copies = begin(pairs + [(down_w, downs)], sems)
    else:
        *ys, rows_ref = rest
        width = gate_w.shape[0] // chunks
        downs = down_w
    gate = up = None
    for s in range(chunks):
        part = xs[0].shape[0]
        at = pl.ds(pl.multiple_of((ti ^ s) * width, width), width)
        if pieces == 1:
            x = xs[0][:, at]
        else:
            for h in range(halves):
                rows_ref[s % 2, h * part : (h + 1) * part, :] = xs[h * pieces + s][...]
            x = rows_ref[s % 2]
        if staged:
            copies[2 * s].wait()
            copies[2 * s + 1].wait()
            wg, wu = gates[s], ups[s]
        else:
            wg, wu = gate_w[at, :], up_w[at, :]
        g = jnp.dot(x, wg, preferred_element_type=jnp.float32)
        u = jnp.dot(x, wu, preferred_element_type=jnp.float32)
        gate = g if gate is None else gate + g
        up = u if up is None else up + u
    hidden = (gate / (1.0 + jnp.exp(-gate)) * up).astype(jnp.bfloat16)
    if staged:
        copies[-1].wait()
    if staged:
        ys[0][...] = jnp.dot(hidden, downs[...], preferred_element_type=jnp.float32).astype(
            jnp.bfloat16
        )
        return
    cols = ys[0].shape[1]

    def block(n):
        at = pl.ds(pl.multiple_of(n * cols, cols), cols)
        above, below = halves_of(jnp.dot(hidden, downs[:, at], preferred_element_type=jnp.float32))
        if not extra:
            return [above], [below]
        more_above, more_below = halves_of(added[:, at])
        return [above, more_above], [below, more_below]

    spread_out(block, ti, ys, direct)


def out_shapes(rows, cols, tp, direct):
    return [sds((rows, cols))] * (tp if direct else 4)


def run_expert(xs, halves, gate_w, up_w, down_w, tp, direct, extra=()):
    rows = xs[0].shape[0] * halves
    width, hidden = gate_w.shape
    pieces = len(xs) // halves
    staged = pieces == 1
    if staged:
        shapes = [sds((rows, down_w.shape[1]))]
    else:
        total = rows + sum(x.shape[0] for x in extra)
        shapes = out_shapes(total, down_w.shape[1] // tp, tp, direct)
    scratch = [pltpu.VMEM((2, rows, width // tp), jnp.bfloat16)]
    if staged:
        part = pltpu.VMEM((tp, width // tp, hidden), jnp.bfloat16)
        scratch += [part, part, pltpu.VMEM(down_w.shape, jnp.bfloat16), DMA((2 * tp + 1,))]
        gate_w, up_w, down_w = far(gate_w), far(up_w), far(down_w)
    return pl.pallas_call(
        lambda *refs: expert_kernel(
            *refs,
            pieces=pieces,
            halves=halves,
            direct=direct,
            staged=staged,
            extra=len(extra) > 0,
        ),
        out_shape=shapes,
        in_specs=[VM] * (len(extra) + len(xs)) + [FAR if staged else VM] * 3,
        out_specs=[VM] * len(shapes),
        scratch_shapes=scratch,
        cost_estimate=cost(6 * rows * width * hidden),
        compiler_params=limit(24),
    )(*extra, *xs, gate_w, up_w, down_w)


def picks_kernel(slots, weights, scale, *picks):
    tokens, width = picks[0].shape
    at = lax.broadcasted_iota(jnp.int32, (tokens, width), 1)
    for k, pick in enumerate(picks):
        own = at == column(slots[k : k + 1, :])
        pick[...] = own.astype(jnp.float32).astype(jnp.bfloat16)
        scale[:, k : k + 1] = column(weights[k : k + 1, :])


def finish_kernel(scale, *refs, count, sums):
    picks, refs = refs[:TOP_K], refs[TOP_K:]
    back, shared, refs = refs[:count], refs[count : count + 2], refs[count + 2 :]
    out = refs[len(sums)]
    rows = jnp.concatenate([part[...] for part in back], axis=0)
    total = jnp.concatenate([part[...] for part in shared], axis=0)
    routed = None
    for k, pick in enumerate(picks):
        term = jnp.dot(pick[...], rows, preferred_element_type=jnp.float32)
        term = scale[:, k : k + 1] * term
        routed = term if routed is None else routed + term
    out[...] = (routed + total).astype(jnp.bfloat16)
    if sums:
        mixed = refs[len(sums) + 1]
        half = mixed.shape[0] // 2
        assert len(sums) == 6
        for n in range(2):
            keep, got, mid = (ref[:half, :].astype(jnp.float32) for ref in refs[3 * n : 3 * n + 3])
            mixed[n * half : (n + 1) * half, :] = (keep + got + mid).astype(jnp.bfloat16)


def rope_kernel(q_far, k_far, v_far, cosine, sine, *refs, size):
    *outs, q, k, v, sems = refs
    copies = begin(((q_far, q), (k_far, k), (v_far, v)), sems)
    z = place()[0]
    rows = q.shape[0]
    both = cosine.shape[1]
    half = size // 2
    lane = lax.broadcasted_iota(jnp.int32, (rows, both), 1)
    front = (lane % size) < half
    c, s_ = cosine[...], sine[...]
    for copy in copies:
        copy.wait()
    for s, out in enumerate(outs):
        at = pl.ds(pl.multiple_of((z ^ s) * both, both), both)
        for n, ref in enumerate((q, k)):
            x = ref[:, at].astype(jnp.float32)
            turned = jnp.where(front, pltpu.roll(x, both - half, 1), pltpu.roll(x, half, 1))
            out[n * rows : (n + 1) * rows, :] = (x * c + turned * s_).astype(jnp.bfloat16)
        out[2 * rows : 3 * rows, :] = v[:, at]


def attend_kernel(lam_far, gain_far, *refs, count, rows, size):
    own, other, outs = refs[:count], refs[count : 2 * count], refs[2 * count : 3 * count]
    qs, ks, vs, scores, weights, heads, lam, gain, sems = refs[3 * count :]
    z, core, _ = place()
    both = 2 * size
    value = vs.shape[1] // 2
    keys = 2 * rows
    pairs = [(lam_far, lam), (gain_far, gain)]
    for s in range(count):
        at = pl.multiple_of((z ^ s) * rows, rows)
        mine = pl.multiple_of((2 * (z ^ s) + core) * rows, rows)
        theirs = pl.multiple_of((2 * (z ^ s) + 1 - core) * rows, rows)
        pairs.append((own[s].at[pl.ds(0, rows), :], qs.at[pl.ds(at, rows), :]))
        for ref, to in ((own[s], mine), (other[s], theirs)):
            k_rows, v_rows, to = pl.ds(rows, rows), pl.ds(2 * rows, rows), pl.ds(to, rows)
            pairs.append((ref.at[k_rows, :], ks.at[to, :]))
            pairs.append((ref.at[v_rows, :], vs.at[to, pl.ds(0, value)]))
    copies = begin(pairs, sems)
    vs[:, value:] = jnp.ones((vs.shape[0], value), jnp.bfloat16)
    for copy in copies:
        copy.wait()
    factor = LOG2E * size ** (-0.5)
    lane = lax.broadcasted_iota(jnp.int32, (rows, both), 1)
    tile = math.gcd(rows, 64)
    ahead = lax.broadcasted_iota(jnp.int32, (tile, keys), 1) - lax.broadcasted_iota(
        jnp.int32, (tile, keys), 0
    )
    contract = (((1,), (1,)), ((), ()))
    units = [(block, m) for block in reversed(range(count)) for m in range(2)]
    maps = {}

    def score(u):
        block, m = units[u]
        q = qs[block * rows : (block + 1) * rows, :]
        q = jnp.where((lane < size) == (m == 0), q, jnp.zeros_like(q))
        for j in range(block + 1):
            at = slice(j * keys, (j + 1) * keys)
            scores[u % 2, :, at] = lax.dot_general(
                q, ks[at, :], contract, preferred_element_type=jnp.float32
            )

    def weigh(u):
        block, _ = units[u]
        for r in range(0, rows, tile):
            pieces = []
            for j in range(block + 1):
                piece = scores[u % 2, r : r + tile, j * keys : (j + 1) * keys]
                if j == block:
                    piece = jnp.where(ahead <= core * rows + r, piece, masked_low)
                pieces.append(piece)
            top = None
            for piece in pieces:
                one = jnp.max(piece, axis=1, keepdims=True)
                top = one if top is None else jnp.maximum(top, one)
            for j, piece in enumerate(pieces):
                weights[u % 2, r : r + tile, j * keys : (j + 1) * keys] = jnp.exp2(
                    (piece - top) * factor
                ).astype(jnp.bfloat16)

    def mix(u):
        block, m = units[u]
        span = (block + 1) * keys
        acc = jnp.dot(weights[u % 2, :, :span], vs[:span, :], preferred_element_type=jnp.float32)
        maps[m] = acc[:, :value] / acc[:, value:]
        if m == 1:
            heads_at = lax.broadcasted_iota(jnp.int32, lam.shape, 1)
            factor2 = jnp.sum(jnp.where(heads_at == z, lam[...], 0.0), axis=1, keepdims=True)
            diff = maps[0] - factor2 * maps[1]
            inverse = lax.rsqrt(jnp.mean(diff * diff, axis=1, keepdims=True) + norm_eps)
            heads[block * rows : (block + 1) * rows, :] = (diff * inverse * gain[...]).astype(
                jnp.bfloat16
            )

    score(0)
    for u in range(len(units)):
        if u + 1 < len(units):
            score(u + 1)
        if u > 0:
            mix(u - 1)
        weigh(u)
    mix(len(units) - 1)
    for s in range(count):
        outs[s][...] = heads[pl.ds(pl.multiple_of((z ^ s) * rows, rows), rows), :]


def project_kernel(*refs, count, direct):
    heads, weight, (*outs, rows_ref) = refs[:count], refs[count], refs[count + 1 :]
    z, _, ti = place()
    value = heads[0].shape[1]
    for s in range(count):
        rows_ref[:, pl.ds(pl.multiple_of((z ^ s) * value, value), value)] = heads[s][...]
    rows = rows_ref[...]
    cols = outs[0].shape[1]

    def block(n):
        at = pl.ds(pl.multiple_of(n * cols, cols), cols)
        above, below = halves_of(jnp.dot(rows, weight[:, at], preferred_element_type=jnp.float32))
        return [above], [below]

    spread_out(block, ti, outs, direct)


def rotate(inputs, positions):
    half_size = inputs.shape[-1] // 2
    frequency = theta_base ** (-(jnp.arange(half_size, dtype=jnp.float32) * 2.0) / inputs.shape[-1])
    angles = positions.astype(jnp.float32)[:, None] * frequency[None, :]
    cosine = jnp.cos(angles)[:, None, None, :]
    sine_part = jnp.sin(angles)[:, None, None, :]
    front_half = inputs[..., :half_size]
    back_half = inputs[..., half_size:]
    return jnp.concatenate(
        [front_half * cosine - back_half * sine_part, back_half * cosine + front_half * sine_part],
        axis=-1,
    )


def gathered_attention(query_pairs, key_pairs, value_rows, head_lambda, head_gain):
    local_rows = query_pairs.shape[0]
    local_heads = head_lambda.shape[0]
    head_size = query_pairs.shape[1] // (2 * local_heads)
    value_size = value_rows.shape[1] // local_heads
    positions = lax.axis_index("ep") * local_rows + jnp.arange(local_rows, dtype=jnp.int32)
    rot_queries = rotate(
        query_pairs.astype(jnp.float32).reshape(local_rows, local_heads, 2, head_size), positions
    ).astype(jnp.bfloat16)
    rot_keys = rotate(
        key_pairs.astype(jnp.float32).reshape(local_rows, local_heads, 2, head_size), positions
    ).astype(jnp.bfloat16)
    rot_keys = rot_keys.reshape(local_rows, local_heads * 2 * head_size)
    zero_init = (
        jnp.full((local_heads, 2, local_rows), masked_low, jnp.float32),
        jnp.zeros((local_heads, 2, local_rows), jnp.float32),
        jnp.zeros((local_heads, 2, local_rows, value_size), jnp.float32),
    )
    piece_keys = lax.all_gather(rot_keys, "ep", axis=0, tiled=True)
    piece_values = lax.all_gather(value_rows, "ep", axis=0, tiled=True)
    block_count = piece_keys.shape[0] // KEY_BLOCK
    group_size = 4 if block_count % 4 == 0 else 1
    group_count = block_count // group_size
    grouped_keys = piece_keys.reshape(group_count, group_size, KEY_BLOCK, local_heads, 2, head_size)
    grouped_values = piece_values.reshape(
        group_count, group_size, KEY_BLOCK, local_heads, value_size
    )

    def one_group(current, inputs):
        block_keys, block_values, group_index = inputs
        key_positions = group_index * group_size * KEY_BLOCK + jnp.arange(
            group_size * KEY_BLOCK, dtype=jnp.int32
        ).reshape(group_size, KEY_BLOCK)
        scores = jnp.einsum(
            "qhmd,gkhmd->hmqgk", rot_queries, block_keys, preferred_element_type=jnp.float32
        ) * head_size ** (-0.5)
        allowed = key_positions[None, :, :] <= positions[:, None, None]
        scores = jnp.where(allowed, scores, masked_low)
        block_max = jnp.max(scores, axis=-1)
        weights = jnp.where(allowed, jnp.exp(scores - block_max[..., None]), 0.0)
        block_sum = jnp.sum(weights, axis=-1)
        block_out = jnp.einsum(
            "hmqgk,gkhc->hmqgc",
            weights.astype(jnp.bfloat16),
            block_values,
            preferred_element_type=jnp.float32,
        )
        run_max, run_sum, run_out = current
        new_max = jnp.maximum(run_max, jnp.max(block_max, axis=-1))
        old_scale = jnp.exp(run_max - new_max)
        new_scale = jnp.exp(block_max - new_max[..., None])
        run_sum = run_sum * old_scale + jnp.sum(new_scale * block_sum, axis=-1)
        run_out = run_out * old_scale[..., None] + jnp.sum(
            new_scale[..., None] * block_out, axis=-2
        )
        return ((new_max, run_sum, run_out), None)

    result, _ = lax.scan(
        one_group,
        zero_init,
        (grouped_keys, grouped_values, jnp.arange(group_count, dtype=jnp.int32)),
    )
    _, run_sum, run_out = result
    map_outputs = run_out / run_sum[..., None]
    difference = map_outputs[:, 0] - head_lambda[:, None, None] * map_outputs[:, 1]
    inverse_rms = lax.rsqrt(jnp.mean(difference * difference, axis=-1, keepdims=True) + norm_eps)
    normed_heads = (difference * inverse_rms * head_gain).astype(jnp.bfloat16)
    return [normed_heads.transpose(1, 0, 2).reshape(local_rows, local_heads * value_size)]


def inner(
    query_pairs,
    key_pairs,
    value_rows,
    head_lambda,
    head_gain,
    out_weight,
    moe_input,
    ffn_gain,
    routes,
    route_weight,
    gate_weight,
    up_weight,
    down_weight,
    shared_gate,
    shared_up,
    shared_down,
):
    ep, tp = lax.axis_size("ep"), lax.axis_size("tp")
    chips = ep // 2
    ei = lax.axis_index("ep")

    def along_z(x, s):
        return lax.ppermute(x, "ep", [(i, 2 * ((i // 2) ^ s) + i % 2) for i in range(ep)])

    def swap(x):
        return lax.ppermute(x, "ep", [(i, i ^ 1) for i in range(ep)])

    def along_tp(x, s):
        return lax.ppermute(x, "tp", [(i, i ^ s) for i in range(tp)])

    def exchange(parts, move, near_first=False):
        moved = {}
        turns = range(1, len(parts))
        for s in turns if near_first else reversed(turns):
            moved[s] = move(parts[s], s)
        return [parts[0]] + [moved[s] for s in range(1, len(parts))]

    direct = tp != 4

    def gather_tp(own, other):
        if direct:
            return [
                piece
                for half in (own, other)
                for piece in [half] + [along_tp(half, s) for s in range(1, tp)]
            ]
        own_1, other_2 = along_tp(own, 1), along_tp(other, 2)
        own_2, other_1 = along_tp(own, 2), along_tp(other, 1)
        own_3, other_3 = along_tp(own_1, 2), along_tp(other_2, 1)
        return [own, own_1, own_2, own_3, other, other_1, other_2, other_3]

    def reduce_tp(parts, open_end=False):
        up = lambda x: x.astype(jnp.float32)
        if direct:
            total = sum(up(p) for p in exchange(parts, along_tp))
            half = total.shape[0] // 2
            return total[:half], total[half:]
        send_x, keep_x, send_y, keep_y = parts
        half = send_x.shape[0] // 2
        if open_end:
            far_x, far_y = along_tp(send_x[half:], 1), along_tp(send_y[half:], 2)
            got_x, got_y = along_tp(send_x[:half], 1), along_tp(send_y[:half], 2)
            mid_x = (up(keep_x[half:]) + up(far_x)).astype(jnp.bfloat16)
            mid_y = (up(keep_y[half:]) + up(far_y)).astype(jnp.bfloat16)
            mid_x, mid_y = along_tp(mid_x, 2), along_tp(mid_y, 1)
            return [keep_x, got_x, mid_x, keep_y, got_y, mid_y]
        got_x, got_y = along_tp(send_x, 1), along_tp(send_y, 2)
        mid_x = (up(keep_x[half:]) + up(got_x[half:])).astype(jnp.bfloat16)
        mid_y = (up(keep_y[half:]) + up(got_y[half:])).astype(jnp.bfloat16)
        mid_x, mid_y = along_tp(mid_x, 2), along_tp(mid_y, 1)
        return (
            up(keep_x[:half]) + up(got_x[:half]) + up(mid_x),
            up(keep_y[:half]) + up(got_y[:half]) + up(mid_y),
        )

    tokens, width = moe_input.shape
    cap = tokens * TOP_K * 5 // (4 * ep)
    slice_width = width // tp
    xn, slots, *parts = pl.pallas_call(
        lambda *refs: dispatch_kernel(*refs, cap=cap, experts=ep),
        out_shape=[sds((tokens, width)), sds((TOP_K, tokens), jnp.int32)]
        + [sds((2 * cap, slice_width))] * chips,
        in_specs=[FAR] * 3,
        out_specs=[VM] * (2 + chips),
        scratch_shapes=[
            pltpu.VMEM(moe_input.shape, jnp.bfloat16),
            pltpu.VMEM((1, width), jnp.float32),
            pltpu.VMEM((TOP_K, tokens), jnp.int32),
            DMA((3,)),
        ],
        cost_estimate=cost(4e8),
        name="dispatch",
        compiler_params=limit(8),
    )(far(moe_input), far(ffn_gain.reshape(1, -1)), far(routes.T))
    arrived = exchange(parts, along_z)
    picks = pl.pallas_call(
        picks_kernel,
        out_shape=[sds((tokens, TOP_K), jnp.float32)] + [sds((tokens, ep * cap))] * TOP_K,
        in_specs=[VM] * 2,
        out_specs=[VM] * (1 + TOP_K),
        cost_estimate=cost(1e8),
        compiler_params=limit(8),
        name="picks",
    )(slots, route_weight.T)

    rows = query_pairs.shape[0]
    heads = head_lambda.shape[0]
    size = query_pairs.shape[1] // (2 * heads)
    value = value_rows.shape[1] // heads
    spread = heads == chips and value == 2 * size and value % 128 == 0
    if spread:
        positions = (ei * rows + jnp.arange(rows, dtype=jnp.int32)).astype(jnp.float32)
        index = jnp.arange(2 * size, dtype=jnp.int32)
        frequency = theta_base ** (-((index % (size // 2)).astype(jnp.float32) * 2.0) / size)
        angles = positions[:, None] * frequency[None, :]
        sign = jnp.where(index % size < size // 2, -1.0, 1.0).astype(jnp.float32)
        cosine = jnp.cos(angles)
        sine = jnp.sin(angles) * sign
        packs = pl.pallas_call(
            lambda *refs: rope_kernel(*refs, size=size),
            out_shape=[sds((3 * rows, value))] * chips,
            in_specs=[FAR] * 3 + [VM] * 2,
            out_specs=[VM] * chips,
            scratch_shapes=[pltpu.VMEM(query_pairs.shape, jnp.bfloat16)] * 3 + [DMA((3,))],
            cost_estimate=cost(4e8),
            name="rope",
        compiler_params=limit(8),
        )(far(query_pairs), far(key_pairs), far(value_rows), cosine, sine)
        packs = exchange(packs, along_z, near_first=True)
        others = [swap(packs[0])]
        for s in range(1, chips):
            others.append(swap(packs[s]))

    shared = run_expert([xn], 1, shared_gate, shared_up, shared_down, tp, True)
    own, other = pl.pallas_call(
        lambda *refs: pack_kernel(*refs, count=chips, cap=cap),
        out_shape=[sds((chips * cap, slice_width))] * 2,
        in_specs=[VM] * chips,
        out_specs=[VM] * 2,
        cost_estimate=cost(1e8),
        compiler_params=limit(8),
        name="pack",
    )(*arrived)
    other = swap(other)
    slices = gather_tp(own, other)
    terms = run_expert(
        slices, 2, gate_weight[0], up_weight[0], down_weight[0], tp, direct, extra=shared
    )
    summed = reduce_tp(terms)
    routed = chips * cap
    shared = [x[routed:] for x in summed]
    summed = [x[:routed].astype(jnp.bfloat16) for x in summed]

    sums = []
    if spread:
        heads_out = pl.pallas_call(
            lambda *refs: attend_kernel(*refs, count=chips, rows=rows, size=size),
            out_shape=[sds((rows, value))] * chips,
            in_specs=[FAR, FAR] + [ANY] * (2 * chips),
            out_specs=[VM] * chips,
            scratch_shapes=[
                pltpu.VMEM((chips * rows, value), jnp.bfloat16),
                pltpu.VMEM((ep * rows, value), jnp.bfloat16),
                pltpu.VMEM((ep * rows, 2 * value), jnp.bfloat16),
                pltpu.VMEM((2, rows, ep * rows), jnp.float32),
                pltpu.VMEM((2, rows, ep * rows), jnp.bfloat16),
                pltpu.VMEM((chips * rows, value), jnp.bfloat16),
                pltpu.VMEM((1, heads), jnp.float32),
                pltpu.VMEM((1, value), jnp.float32),
                DMA((5 * chips + 2,)),
            ],
            cost_estimate=cost(4e9),
            name="attend",
        compiler_params=limit(32),
        )(head_lambda.reshape(1, -1), head_gain.reshape(1, -1), *packs, *others)
        normed = exchange(heads_out, along_z)
        cols = out_weight.shape[1] // tp
        shapes = out_shapes(rows, cols, tp, direct)
        mixer = pl.pallas_call(
            lambda *refs: project_kernel(*refs, count=chips, direct=direct),
            out_shape=shapes,
            in_specs=[VM] * (chips + 1),
            out_specs=[VM] * len(shapes),
            scratch_shapes=[pltpu.VMEM((rows, chips * value), jnp.bfloat16)],
            cost_estimate=cost(1e9),
            name="project",
            compiler_params=limit(12),
        )(*normed, out_weight)
        sums = reduce_tp(mixer, open_end=not direct)
        if direct:
            attn_out = jnp.concatenate(sums, axis=0).astype(jnp.bfloat16)
            sums = []
    else:
        head_rows = gathered_attention(query_pairs, key_pairs, value_rows, head_lambda, head_gain)[0]
        mixer = jnp.dot(head_rows, out_weight, preferred_element_type=jnp.float32)
        attn_out = lax.psum_scatter(
            mixer.astype(jnp.bfloat16), "tp", scatter_dimension=1, tiled=True
        )

    back = swap(summed[1])
    groups = [
        jnp.concatenate([x[s * cap : (s + 1) * cap] for x in (summed[0], back)], axis=0)
        for s in range(chips)
    ]
    groups = exchange(groups, along_z)
    outs = [sds((tokens, slice_width))]
    if sums:
        outs.append(sds((rows, cols)))
    finished = pl.pallas_call(
        lambda *refs: finish_kernel(*refs, count=chips, sums=sums),
        out_shape=outs,
        in_specs=[VM] * (1 + TOP_K + chips + len(shared) + len(sums)),
        out_specs=[VM] * len(outs),
        cost_estimate=cost(4e8),
        compiler_params=limit(12),
        name="finish",
    )(*picks, *groups, *shared, *sums)
    moe_out = finished[0]
    if sums:
        attn_out = finished[1]
    return (attn_out, moe_out)


def solution(mesh):
    return jax.shard_map(
        inner,
        mesh=mesh,
        in_specs=(
            P("ep", "tp"),
            P("ep", "tp"),
            P("ep", "tp"),
            P("tp"),
            P(),
            P("tp", None),
            P("ep", None),
            P(),
            P("ep", None),
            P("ep", None),
            P("ep", None, "tp"),
            P("ep", None, "tp"),
            P("ep", "tp", None),
            P(None, "tp"),
            P(None, "tp"),
            P("tp", None),
        ),
        out_specs=(P("ep", "tp"), P("ep", "tp")),
        check_vma=False,
    )
```
